768 devices in a mesh: ep: 48 (over z, x), tp: 16 (over y, core).
Axes of the slice: x: 4, y: 8, z: 12, core: 2. Of those that a mesh axis runs over, the one named last changes fastest.
Arguments:
- tokens: bfloat16 [1152, 2048], P('ep'), may hold values from -12 to 12
- state: float32 [1152, 16, 128, 256], P('ep', 'tp'), may hold values from -6 to 6
- w_query: bfloat16 [2048, 2048], P(None, 'tp'), may hold values from -0.125 to 0.125
- w_key: bfloat16 [2048, 2048], P(None, 'tp'), may hold values from -0.125 to 0.125
- w_value: bfloat16 [2048, 4096], P(None, 'tp'), may hold values from -0.125 to 0.125
- w_outgate: bfloat16 [2048, 4096], P(None, 'tp'), may hold values from -0.125 to 0.125
- decay_down: bfloat16 [2048, 16], replicated, may hold values from -0.125 to 0.125
- decay_up: bfloat16 [16, 2048], P(None, 'tp'), may hold values from -9 to 9
- decay_bias: float32 [2048], P('tp'), may hold values from -6 to 4
- head_gain: float32 [256], replicated, may hold values from 0.1 to 1.9
- w_output: bfloat16 [4096, 2048], P('tp'), may hold values from -0.09375 to 0.09375
- norm1_gain: float32 [2048], P('tp'), may hold values from 0.1 to 1.9
- route_ids: int32 [1152, 6], P('ep'), may hold values from 0 to 191, all different within a row; in each aligned block of 24 rows (0 to 23, 24 to 47, ...) at most 2 rows name the same one
- route_weight: float32 [1152, 6], P('ep'), may hold values from 0.1 to 1
- exp_gate: bfloat16 [192, 2048, 512], P('ep', 'tp'), may hold values from -0.125 to 0.125
- exp_up: bfloat16 [192, 2048, 512], P('ep', 'tp'), may hold values from -0.125 to 0.125
- exp_down: bfloat16 [192, 512, 2048], P('ep', None, 'tp'), may hold values from -0.25 to 0.25
- sh_gate: bfloat16 [2048, 512], P('tp'), may hold values from -0.125 to 0.125
- sh_up: bfloat16 [2048, 512], P('tp'), may hold values from -0.125 to 0.125
- sh_down: bfloat16 [512, 2048], P(None, 'tp'), may hold values from -0.25 to 0.25
- norm2_gain: float32 [2048], P('tp'), may hold values from 0.1 to 1.9
Outputs:
- layer_out: bfloat16 [1152, 2048], P('ep', 'tp')
The draws below stay inside these ranges and needn't reach their ends.
Inputs may be any that keep to these rules, and one draw needn't show every extreme that they name: `route_ids`: each row names 6 different experts. Among the rows of one index of ep (aligned blocks of 24 rows) no expert is named by more than 2 rows, and in some blocks one expert is named by exactly 2.
All inputs are finite; a program needn't handle non-finite values.
Results may differ from the reference program's by a relative error of at most 0.02.
Values may be sent and summed in bfloat16 or wider, within the bound.
No kernel may reach another device: no remote copies, remote signals or barrier semaphores. Data moves between devices by JAX's collectives and lax.ppermute only.
A program may use at most 32 MiB of HBM per device.

```python
import math
import jax
import jax.numpy as jnp
import numpy as np
from jax import lax

D = 2048
HEADS = 16
KEY_DIM = 128
VAL_DIM = 256
RANK = 16
FF_EXP = 512
FF_SHARED = 512
TOPK = 6
TOK_DEV = 24
BATCH = 1152
EXPERTS = 192
CAP = 2
N_EP = 48
N_TP = 16


def draw_tokens(key, part):
    column = jnp.arange(D, dtype=jnp.float32) / D
    ramp = jnp.exp((2.0 * column - 1.0) * jnp.log(3.0))
    drawn = jax.random.normal(key, (BATCH, D), jnp.float32) * ramp
    return jnp.clip(drawn, -12.0, 12.0).astype(jnp.bfloat16)


def block_scale(stream_key, dims, cuts, smallest, top_value):
    loudness, own = 1.0, jax.random.fold_in(stream_key, 6)
    for axis_at, shards_of in cuts:
        heights = jnp.exp(jax.random.uniform(jax.random.fold_in(own, axis_at), (shards_of,), jnp.float32, smallest / len(cuts), top_value / len(cuts)))
        loudness = loudness * jnp.repeat(heights, dims[axis_at] // shards_of).reshape([-1 if axis == axis_at else 1 for axis in range(len(dims))])
    return loudness


def assign_block(rng, own, number, rows, number_of, top, limit, lean):
    sequence = jax.random.permutation(rng, number_of)
    heavy_load, common = load_shares(number_of, rows * top, limit, lean, True), load_shares(number_of, rows * top, limit, lean, False)
    places = jnp.arange(number_of)

    def named(lengths, turn):
        used = int((lengths > 0).sum())
        fixed = max(1, used // 4)
        moved = fixed + (places - fixed + turn * (used - fixed)) % max(1, number_of - fixed)
        return jnp.zeros((number_of,), jnp.int32).at[sequence[jnp.where(places < fixed, places, moved)]].set(jnp.asarray(lengths, jnp.int32))

    lengths = jnp.where(number % 4 == 0, named(heavy_load, number // 4), named(common, number - number // 4 - 1))
    mixed = jax.random.permutation(jax.random.fold_in(own, 3), number_of)
    giver, sink = mixed[0:number_of // 2 * 2:2], mixed[1:number_of // 2 * 2:2]
    margin = jnp.minimum(lengths[giver] - 1, limit - lengths[sink]) // 2
    margin = jnp.where((giver == sequence[0]) | (sink == sequence[0]) | (lengths[sink] == 0), 0, jnp.maximum(margin, 0))
    moved = jax.random.randint(jax.random.fold_in(own, 4), (number_of // 2,), 0, 1 << 20) % (margin + 1)
    lengths = lengths.at[giver].add(-moved).at[sink].add(moved)
    members = jnp.searchsorted(jnp.cumsum(lengths), jnp.arange(rows * top), side="right").astype(jnp.int32)
    listing = members.reshape(top, rows).T
    listing = listing[jax.random.permutation(jax.random.fold_in(own, 1), rows)]
    turn = jax.random.randint(jax.random.fold_in(own, 2), (rows, 1), 0, top)
    return jnp.take_along_axis(listing, (jnp.arange(top)[None, :] + turn) % top, axis=1)


def load_shares(count, total, reach, skew, full):
    weights = [(1 << 20) // math.isqrt(grade ** skew) + 1 for grade in range(1, count + 1)]
    largest = reach if full else min(reach, max(-(-total // count), total * weights[0] // sum(weights)))
    least = 1 if total - largest >= count - 1 else 0
    holding, spare = [largest] + [least] * (count - 1), total - largest - least * (count - 1)
    while spare > 0:
        movable = [i for i in range(1, count) if holding[i] < largest] or [i for i in range(1, count) if holding[i] < reach]
        whole, remaining = sum([weights[i] for i in movable]), spare
        for i in movable:
            more = min(reach - holding[i], max(1, remaining * weights[i] // whole), spare)
            holding[i] = holding[i] + more
            spare = spare - more
    return np.array(holding)


def noise(stream_key, extent, scale, limit, cuts=(), kind=jnp.bfloat16):
    loudness = block_scale(stream_key, extent, cuts, -0.22, 0.18) if cuts else 1.0
    values = jax.random.normal(stream_key, extent, jnp.float32) * scale * loudness
    return jnp.minimum(jnp.maximum(values, -limit), limit).astype(kind)


def setup_inputs(seed: int = 0) -> dict:
    keys = jax.random.split(jax.random.key(seed), 22)
    tokens = draw_tokens(jax.random.fold_in(keys[21], 71), 0)
    state = noise(keys[1], (BATCH, HEADS, KEY_DIM, VAL_DIM), 1.0, 6.0, ((0, 48), (1, 16)), jnp.float32)
    w_query = noise(keys[2], (D, HEADS * KEY_DIM), D ** -0.5, 0.125, ((1, 16),))
    w_key = noise(keys[3], (D, HEADS * KEY_DIM), D ** -0.5, 0.125, ((1, 16),))
    w_value = noise(keys[4], (D, HEADS * VAL_DIM), D ** -0.5, 0.125, ((1, 16),))
    w_outgate = noise(keys[5], (D, HEADS * VAL_DIM), D ** -0.5, 0.125, ((1, 16),))
    decay_down = noise(keys[6], (D, RANK), D ** -0.5, 0.125)
    decay_up = noise(keys[7], (RANK, HEADS * KEY_DIM), 1.5, 9.0, ((1, 16),))
    decay_bias = jnp.clip(-6.0 + 10.0 * jax.random.uniform(keys[8], (HEADS * KEY_DIM,), jnp.float32) ** block_scale(keys[8], (HEADS * KEY_DIM,), ((0, 16),), -0.2, 0.2), -6.0, 4.0)
    head_gain = jnp.clip(1.0 + 0.18 * jax.random.normal(keys[9], (VAL_DIM,), jnp.float32), 0.1, 1.9)
    w_output = noise(keys[10], (HEADS * VAL_DIM, D), (HEADS * VAL_DIM) ** -0.5, 0.09375, ((0, 16),))
    norm1_gain = jnp.clip(1.0 + 0.18 * jax.random.normal(keys[11], (D,), jnp.float32), 0.1, 1.9)
    route_ids_keys = jax.random.split(jax.random.fold_in(keys[12], 1), BATCH // TOK_DEV)
    route_ids_turns = jax.random.permutation(jax.random.fold_in(keys[12], 3), BATCH // TOK_DEV)
    route_ids = jax.vmap(lambda own, number: assign_block(jax.random.fold_in(keys[12], 2), own, number, TOK_DEV, EXPERTS, TOPK, CAP, 2))(route_ids_keys, route_ids_turns).reshape((BATCH, TOPK))
    route_weight = jnp.clip(0.1 + 0.9 * jax.random.uniform(keys[13], (BATCH, TOPK), jnp.float32) ** block_scale(keys[13], (BATCH, TOPK), ((0, 48),), -0.2, 0.2), 0.1, 1.0)
    exp_gate = noise(keys[14], (EXPERTS, D, FF_EXP), D ** -0.5, 0.125, ((0, 48), (1, 16)))
    exp_up = noise(keys[15], (EXPERTS, D, FF_EXP), D ** -0.5, 0.125, ((0, 48), (1, 16)))
    exp_down = noise(keys[16], (EXPERTS, FF_EXP, D), FF_EXP ** -0.5, 0.25, ((0, 48), (2, 16)))
    sh_gate = noise(keys[17], (D, FF_SHARED), D ** -0.5, 0.125, ((0, 16),))
    sh_up = noise(keys[18], (D, FF_SHARED), D ** -0.5, 0.125, ((0, 16),))
    sh_down = noise(keys[19], (FF_SHARED, D), FF_SHARED ** -0.5, 0.25, ((1, 16),))
    norm2_gain = jnp.clip(1.0 + 0.18 * jax.random.normal(keys[20], (D,), jnp.float32), 0.1, 1.9)
    return dict(tokens=tokens, state=state, w_query=w_query, w_key=w_key, w_value=w_value, w_outgate=w_outgate, decay_down=decay_down, decay_up=decay_up, decay_bias=decay_bias, head_gain=head_gain, w_output=w_output, norm1_gain=norm1_gain, route_ids=route_ids, route_weight=route_weight, exp_gate=exp_gate, exp_up=exp_up, exp_down=exp_down, sh_gate=sh_gate, sh_up=sh_up, sh_down=sh_down, norm2_gain=norm2_gain)


res_scale = 2.0 ** 0.5
decay_tau = 16.0
norm_eps = 1e-05

def settle(values):
    return lax.optimization_barrier(values.astype(jnp.bfloat16)).astype(jnp.float32)

def project(left, right):
    return jnp.dot(left, right, preferred_element_type=jnp.float32)

def grouped_sum(left, right, group_count):
    width = right.shape[0] // group_count

    def add_group(running, group_index):
        left_piece = lax.dynamic_slice_in_dim(left, group_index * width, width, 1)
        right_block = lax.dynamic_slice_in_dim(right, group_index * width, width, 0)
        return (running + settle(project(left_piece, right_block)), None)
    start = jnp.zeros((left.shape[0], right.shape[1]), jnp.float32)
    running, _ = lax.scan(add_group, start, jnp.arange(group_count, dtype=jnp.int32))
    return running

def layer_norm(values, gain):
    center = values - lax.optimization_barrier(jnp.mean(values, -1, keepdims=True))
    spread = lax.optimization_barrier(jnp.mean(center * center, -1, keepdims=True))
    return center * lax.rsqrt(spread + norm_eps) * gain

def reference(tokens, state, w_query, w_key, w_value, w_outgate, decay_down, decay_up, decay_bias, head_gain, w_output, norm1_gain, route_ids, route_weight, exp_gate, exp_up, exp_down, sh_gate, sh_up, sh_down, norm2_gain):
    queries = settle(project(tokens, w_query)).reshape(BATCH, HEADS, KEY_DIM) * KEY_DIM ** (-0.5)
    key_rows = settle(project(tokens, w_key)).reshape(BATCH, HEADS, KEY_DIM)
    values = settle(project(tokens, w_value)).reshape(BATCH, HEADS, VAL_DIM)
    gate_pre = settle(project(tokens, w_outgate)).reshape(BATCH, HEADS, VAL_DIM)
    decay_low = lax.optimization_barrier(project(tokens, decay_down).astype(jnp.bfloat16))
    log_decay = (jax.nn.log_sigmoid(project(decay_low, decay_up) + decay_bias) / decay_tau).reshape(BATCH, HEADS, KEY_DIM)
    carried = jnp.einsum('bhk,bhkv->bhv', queries * jnp.exp(log_decay), state, precision=lax.Precision.HIGHEST)
    attended = carried + lax.optimization_barrier(jnp.sum(queries * key_rows, -1, keepdims=True)) * values
    inv_norm = lax.rsqrt(lax.optimization_barrier(jnp.mean(attended * attended, -1, keepdims=True)) + norm_eps)
    head_out = (attended * inv_norm * head_gain * jax.nn.silu(gate_pre)).astype(jnp.bfloat16).reshape(BATCH, HEADS * VAL_DIM)
    mixed = settle(grouped_sum(head_out, w_output, N_TP))
    normed_mid = layer_norm(res_scale * tokens.astype(jnp.float32) + mixed, norm1_gain)
    normed_mid = lax.optimization_barrier(normed_mid.astype(jnp.bfloat16))
    pair_count = TOK_DEV * TOPK
    expert_ids = route_ids.reshape(N_EP, pair_count)
    onehot = (expert_ids[:, :, None] == jnp.arange(EXPERTS, dtype=jnp.int32)[None, None, :]).astype(jnp.int32)
    ranks = lax.optimization_barrier(jnp.sum((jnp.cumsum(onehot, 1) - 1) * onehot, -1))
    group_ids = jnp.arange(N_EP, dtype=jnp.int32)[:, None]
    positions = (expert_ids * (N_EP * CAP) + group_ids * CAP + ranks).reshape(BATCH * TOPK)
    token_ids = jnp.arange(BATCH * TOPK, dtype=jnp.int32) // TOPK
    table = jnp.full((EXPERTS * N_EP * CAP,), BATCH, jnp.int32).at[positions].set(token_ids)
    padded = jnp.concatenate([normed_mid, jnp.zeros((1, D), jnp.bfloat16)], 0)

    def one_expert(operands):
        row_ids, gate_weight, up_weight, down_weight = operands
        chosen = padded[row_ids]
        gate_sum = settle(grouped_sum(chosen, gate_weight, N_TP))
        up_sum = settle(grouped_sum(chosen, up_weight, N_TP))
        inner = (jax.nn.silu(gate_sum) * up_sum).astype(jnp.bfloat16)
        return project(inner, down_weight).astype(jnp.bfloat16)
    expert_out = lax.map(one_expert, (table.reshape(EXPERTS, N_EP * CAP), exp_gate, exp_up, exp_down))
    expert_out = expert_out.reshape(EXPERTS * N_EP * CAP, D)
    picked = expert_out[positions].astype(jnp.float32).reshape(BATCH, TOPK, D)
    routed = lax.optimization_barrier(jnp.sum(picked * route_weight[:, :, None], 1))
    shared_gate = settle(grouped_sum(normed_mid, sh_gate, N_TP))
    shared_up = settle(grouped_sum(normed_mid, sh_up, N_TP))
    shared_inner = (jax.nn.silu(shared_gate) * shared_up).astype(jnp.bfloat16)
    mixture = routed + project(shared_inner, sh_down)
    return layer_norm(res_scale * normed_mid.astype(jnp.float32) + mixture, norm2_gain).astype(jnp.bfloat16)
```

```python
import jax
import jax.numpy as jnp
from jax import lax
from jax.experimental import pallas as pl
from jax.experimental.pallas import tpu as pltpu
from jax.sharding import PartitionSpec as P

res_scale = 2.0**0.5
decay_tau = 16.0
norm_eps = 1e-05
capacity = 2
lanes = 128

f32 = jnp.float32
bf16 = jnp.bfloat16


def local_call(body, outs, args, unread=0):
    vmem = pl.BlockSpec(memory_space=pltpu.VMEM)
    anywhere = pl.BlockSpec(memory_space=pl.ANY)
    return pl.pallas_call(
        body,
        out_shape=outs,
        in_specs=[vmem] * (len(args) - unread) + [anywhere] * unread,
        out_specs=jax.tree.map(lambda _: vmem, outs),
        name=body.__name__,
    )(*args)


def struct(shape, dtype):
    return jax.ShapeDtypeStruct(shape, dtype)


def iota(shape, dim):
    return lax.broadcasted_iota(jnp.int32, shape, dim)


def dot(left, right):
    return jnp.dot(left, right, preferred_element_type=f32)


def rounded(value):
    return value.astype(bf16).astype(f32)


def as_row(column):
    rows = column.shape[0]
    seen = jnp.where(iota((rows, lanes), 0) == iota((rows, lanes), 1), column, 0.0)
    return jnp.sum(seen, axis=0, keepdims=True)


def as_column(row, rows):
    seen = jnp.where(iota((rows, lanes), 0) == iota((rows, lanes), 1), row, 0.0)
    return jnp.sum(seen, axis=1, keepdims=True)


def silu(value):
    return value * jax.nn.sigmoid(value)


def attend(
    tok_ref, state_ref, wq_ref, wk_ref, wv_ref, wg_ref, dd_ref, du_ref, db_ref, hg_ref, wo_ref, out_ref
):
    rows = tok_ref.shape[0]
    key_dim = wq_ref.shape[1]
    tok = tok_ref[...]
    queries = rounded(dot(tok, wq_ref[...])) * key_dim ** (-0.5)
    keys = rounded(dot(tok, wk_ref[...]))
    values = rounded(dot(tok, wv_ref[...]))
    gate = rounded(dot(tok, wg_ref[...]))
    low = dot(tok, dd_ref[...]).astype(bf16)
    pre = dot(low, du_ref[...]) + db_ref[...]
    log_decay = (jnp.minimum(pre, 0.0) - jnp.log1p(jnp.exp(-jnp.abs(pre)))) / decay_tau
    decayed = queries * jnp.exp(log_decay)
    turned = jnp.concatenate([decayed, jnp.zeros((lanes - rows, key_dim), f32)], axis=0).T
    carried = jnp.concatenate(
        [
            jnp.sum(turned[:, b : b + 1] * state_ref[b, 0], axis=0, keepdims=True)
            for b in range(rows)
        ],
        axis=0,
    )
    attended = carried + jnp.sum(queries * keys, axis=1, keepdims=True) * values
    inv_norm = lax.rsqrt(jnp.mean(attended * attended, axis=1, keepdims=True) + norm_eps)
    head_out = (attended * inv_norm * hg_ref[...] * silu(gate)).astype(bf16)
    partial = rounded(dot(head_out, wo_ref[...]))
    row = as_row(jnp.sum(partial, axis=1, keepdims=True))
    high = rounded(row)
    middle = rounded(row - high)
    low = row - high - middle
    at = iota((8, lanes), 0)
    tail = jnp.where(at == 0, high, jnp.where(at == 1, middle, jnp.where(at == 2, low, 0.0)))
    for j in range(out_ref.shape[0]):
        out_ref[j] = jnp.concatenate(
            [partial[:, j * lanes : (j + 1) * lanes], tail], axis=0
        ).astype(bf16)


def place(ids_ref, turned_ref, weight_ref, behind, send_ref, high_ref, low_ref, perm_ref, back_ref):
    rows, top = ids_ref.shape
    slots = send_ref.shape[0]
    blocks = slots // (4 * capacity)
    slot = iota((slots, lanes), 0)
    hit = jnp.zeros((slots, lanes), f32)
    for k in range(top):
        hit = jnp.where(turned_ref[k : k + 1, :] == slot // capacity, 1.0, hit)
    earlier = (iota((lanes, lanes), 0) < iota((lanes, lanes), 1)).astype(bf16)
    rank = dot(hit.astype(bf16), earlier)
    send_ref[...] = jnp.where(rank == (slot % capacity).astype(f32), hit, 0.0).astype(bf16)
    slot = iota((rows, slots), 1)
    hit = jnp.zeros((rows, slots), f32)
    weight = jnp.zeros((rows, slots), f32)
    for k in range(top):
        same = ids_ref[:, k : k + 1] == slot // capacity
        hit = jnp.where(same, 1.0, hit)
        weight = jnp.where(same, weight_ref[:, k : k + 1], weight)
    earlier = (iota((rows, rows), 1) < iota((rows, rows), 0)).astype(bf16)
    rank = dot(earlier, hit.astype(bf16))
    weight = jnp.where(rank == (slot % capacity).astype(f32), weight, 0.0)
    high = weight.astype(bf16)
    high_ref[...] = high
    low_ref[...] = (weight - high.astype(f32)).astype(bf16)
    per_expert = blocks * capacity

    def source(at):
        expert, rest = at // per_expert, at % per_expert
        return rest // capacity * (4 * capacity) + expert * capacity + rest % capacity

    one, two = iota((slots, slots), 0), iota((slots, slots), 1)
    perm_ref[...] = (source(one) == two).astype(bf16)
    back_ref[...] = (one == source(two)).astype(bf16)


def dispatch(got_ref, tok_ref, own_ref, gain_ref, send_ref, rows_ref, centred_ref):
    rows, width = tok_ref.shape
    total = jnp.sum(got_ref[...].astype(f32), axis=0)
    mixed = rounded(total[:rows])
    sums = total[rows : rows + 1] + total[rows + 1 : rows + 2] + total[rows + 2 : rows + 3]
    tok_sum = jnp.sum(tok_ref[...].astype(f32), axis=1, keepdims=True)
    mean = (res_scale * tok_sum + as_column(sums, rows)) / width
    centred = res_scale * own_ref[...].astype(f32) + mixed - mean
    centred_ref[...] = centred
    scaled = centred * gain_ref[...]
    filled = jnp.concatenate([scaled, jnp.zeros((lanes - rows, lanes), f32)], axis=0)
    rows_ref[...] = dot(send_ref[...], filled.astype(bf16)).astype(bf16)


def two_parts(column):
    high = rounded(column)
    return high, column - high


def expand(rows_ref, perm_ref, gate_ref, up_ref, sg_ref, su_ref, gain_ref, centred_ref, out_ref):
    chunks, rows, width = out_ref.shape
    experts, _, hidden = gate_ref.shape
    sorted_rows = dot(perm_ref[...], rows_ref[...])
    scale = sorted_rows / gain_ref[...]
    high, low = two_parts(jnp.sum(scale * scale, axis=1, keepdims=True))
    centred = centred_ref[...]
    own_high, own_low = two_parts(jnp.sum(centred * centred, axis=1, keepdims=True))
    own = (centred * gain_ref[...]).astype(bf16)
    shared_gate, shared_up = dot(own, sg_ref[...]), dot(own, su_ref[...])
    lane = iota((rows, lanes), 1)
    share = hidden // chunks
    per = chunks // experts
    for e in range(experts):
        taken = sorted_rows[e * per * rows : (e + 1) * per * rows].astype(bf16)
        gate, up = dot(taken, gate_ref[e]), dot(taken, up_ref[e])
        for q in range(per):
            j = e * per + q
            cut = slice(q * rows, (q + 1) * rows)
            out_ref[j, :, 0:hidden] = gate[cut].astype(bf16)
            out_ref[j, :, hidden : 2 * hidden] = up[cut].astype(bf16)
            tile = j * share // lanes * lanes
            turn = j * share % lanes
            g = pltpu.roll(shared_gate[:, tile : tile + lanes], (lanes - turn) % lanes, 1)
            u = pltpu.roll(shared_up[:, tile : tile + lanes], (lanes + share - turn) % lanes, 1)
            whole = slice(j * rows, (j + 1) * rows)
            last = jnp.where(lane < share, g, jnp.where(lane < 2 * share, u, 0.0))
            last = jnp.where(lane == 2 * share, high[whole], last)
            last = jnp.where(lane == 2 * share + 1, low[whole], last)
            last = jnp.where(lane == 2 * share + 2, own_high, last)
            last = jnp.where(lane == 2 * share + 3, own_low, last)
            out_ref[j, :, 2 * hidden :] = last.astype(bf16)


def activate(got_ref, inner_ref, own_ref, width):
    chunks, rows, _ = got_ref.shape
    hidden = inner_ref.shape[1] - lanes
    share = hidden // chunks
    total = jnp.sum(got_ref[...].astype(f32), axis=0)
    last = total[:, 2 * hidden :]

    def inv_std(at):
        squares = last[:, at : at + 1] + last[:, at + 1 : at + 2]
        return lax.rsqrt(squares / width + norm_eps)

    inv = inv_std(2 * share)
    gate = rounded(total[:, :hidden] * inv)
    up = rounded(total[:, hidden : 2 * hidden] * inv)
    inner_ref[:, :hidden] = (silu(gate) * up).astype(bf16)
    inv = inv_std(2 * share + 2)
    own_ref[...] = jnp.broadcast_to(inv, own_ref.shape)
    both = rounded(last * inv)
    up = pltpu.roll(both, lanes - share, 1)
    lane = iota((rows, lanes), 1)
    inner_ref[:, hidden:] = jnp.where(lane < share, silu(both) * up, 0.0).astype(bf16)


def contract(inner_ref, back_ref, down_ref, out_ref):
    experts, hidden, _ = down_ref.shape
    per = inner_ref.shape[0] // experts
    outs = [
        dot(inner_ref[e * per : (e + 1) * per, :hidden], down_ref[e]).astype(bf16)
        for e in range(experts)
    ]
    out_ref[...] = dot(back_ref[...], jnp.concatenate(outs, axis=0)).astype(bf16)


def share_out(inner_ref, down_ref, centred_ref, gain_ref, inv_ref, behind, base_ref):
    chunks, _, width = inner_ref.shape
    hidden = width - lanes
    share = hidden // chunks
    normed = rounded(centred_ref[...] * inv_ref[...] * gain_ref[...])
    total = res_scale * normed
    for j in range(chunks):
        total += dot(
            inner_ref[j, :, hidden : hidden + share], down_ref[j * share : (j + 1) * share]
        )
    base_ref[...] = total


def combine(got_ref, high_ref, low_ref, base_ref, resid_ref, stats_ref):
    got = got_ref[...]
    resid = base_ref[...] + dot(high_ref[...], got) + dot(low_ref[...], got)
    resid_ref[...] = resid
    sums = as_row(jnp.sum(resid, axis=1, keepdims=True))
    squares = as_row(jnp.sum(resid * resid, axis=1, keepdims=True))
    at = iota((8, lanes), 0)
    tile = jnp.where(at == 0, sums, jnp.where(at == 1, squares, 0.0))
    for j in range(stats_ref.shape[0]):
        stats_ref[j] = tile


def finish(got_ref, resid_ref, gain_ref, out_ref, width):
    rows = resid_ref.shape[0]
    total = jnp.sum(got_ref[...], axis=0)
    mean = as_column(total[0:1], rows) / width
    spread = as_column(total[1:2], rows) / width - mean * mean
    out_ref[...] = (
        (resid_ref[...] - mean) * lax.rsqrt(spread + norm_eps) * gain_ref[...]
    ).astype(bf16)


def to_each(value, axis):
    return lax.all_to_all(value, axis, split_axis=0, concat_axis=0, tiled=True)


def per_device(
    tokens,
    state,
    w_query,
    w_key,
    w_value,
    w_outgate,
    decay_down,
    decay_up,
    decay_bias,
    head_gain,
    w_output,
    norm1_gain,
    route_ids,
    route_weight,
    exp_gate,
    exp_up,
    exp_down,
    sh_gate,
    sh_up,
    sh_down,
    norm2_gain,
):
    rows, width = tokens.shape
    tp_count, ep_count = lax.axis_size("tp"), lax.axis_size("ep")
    cols = width // tp_count
    hidden = exp_gate.shape[2]
    per_block = exp_gate.shape[0] * capacity
    slots = ep_count * per_block
    gain1, gain2 = norm1_gain.reshape(1, cols), norm2_gain.reshape(1, cols)

    outgoing = local_call(
        attend,
        struct((tp_count, rows + 8, cols), bf16),
        (
            tokens,
            state,
            w_query,
            w_key,
            w_value,
            w_outgate,
            decay_down,
            decay_up,
            decay_bias.reshape(1, -1),
            head_gain.reshape(1, -1),
            w_output,
        ),
    )
    arrived = to_each(outgoing, "tp")
    turned = jnp.pad(route_ids.T, ((0, 2), (0, lanes - rows)), constant_values=-1)
    send, high, low, perm, back = local_call(
        place,
        (
            struct((slots, lanes), bf16),
            struct((rows, slots), bf16),
            struct((rows, slots), bf16),
            struct((slots, slots), bf16),
            struct((slots, slots), bf16),
        ),
        (route_ids, turned, route_weight, outgoing),
        unread=1,
    )
    own_tokens = lax.dynamic_slice_in_dim(tokens, lax.axis_index("tp") * cols, cols, 1)
    sent, centred = local_call(
        dispatch,
        (struct((slots, cols), bf16), struct((rows, cols), f32)),
        (arrived, tokens, own_tokens, gain1, send),
    )
    taken = to_each(sent.reshape(ep_count, per_block, cols), "ep").reshape(slots, cols)
    partials = local_call(
        expand,
        struct((tp_count, rows, 2 * hidden + lanes), bf16),
        (taken, perm, exp_gate, exp_up, sh_gate, sh_up, gain1, centred),
    )
    parts = to_each(partials, "tp")

    def activate_rows(*refs):
        activate(*refs, width)

    activate_rows.__name__ = "activate"
    inner, inv = local_call(
        activate_rows,
        (struct((rows, hidden + lanes), bf16), struct((rows, cols), f32)),
        (parts,),
    )
    inners = lax.all_gather(inner, "tp", axis=0, tiled=True)
    result = local_call(contract, struct((slots, cols), bf16), (inners, back, exp_down))
    returned = to_each(result.reshape(ep_count, per_block, cols), "ep").reshape(slots, cols)
    base = local_call(
        share_out,
        struct((rows, cols), f32),
        (inners.reshape(tp_count, rows, -1), sh_down, centred, gain1, inv, result),
        unread=1,
    )
    resid, stats = local_call(
        combine,
        (struct((rows, cols), f32), struct((tp_count, 8, lanes), f32)),
        (returned, high, low, base),
    )
    all_stats = to_each(stats, "tp")

    def finish_rows(*refs):
        finish(*refs, width)

    finish_rows.__name__ = "finish"
    return local_call(finish_rows, struct((rows, cols), bf16), (all_stats, resid, gain2))


def solution(mesh):
    in_specs = (
        P("ep", None),
        P("ep", "tp", None, None),
        P(None, "tp"),
        P(None, "tp"),
        P(None, "tp"),
        P(None, "tp"),
        P(),
        P(None, "tp"),
        P("tp"),
        P(),
        P("tp", None),
        P("tp"),
        P("ep", None),
        P("ep", None),
        P("ep", "tp", None),
        P("ep", "tp", None),
        P("ep", None, "tp"),
        P("tp", None),
        P("tp", None),
        P(None, "tp"),
        P("tp"),
    )
    out_specs = P("ep", "tp")
    return jax.shard_map(
        per_device, mesh=mesh, in_specs=in_specs, out_specs=out_specs, check_vma=False
    )
```

```python
import jax
import jax.numpy as jnp
from jax import lax
from jax.experimental import pallas as pl
from jax.experimental.pallas import tpu as pltpu
from jax.sharding import PartitionSpec as P

res_scale = 2.0**0.5
decay_tau = 16.0
norm_eps = 1e-05
capacity = 2
lanes = 128

f32 = jnp.float32
bf16 = jnp.bfloat16


def local_call(body, outs, args, stay=(), scratch=()):
    vmem = pl.BlockSpec(memory_space=pltpu.VMEM)
    hbm = pl.BlockSpec(memory_space=pl.ANY)
    placed = [
        pltpu.with_memory_space_constraint(a, pltpu.HBM if k in stay else pltpu.VMEM)
        for k, a in enumerate(args)
    ]
    return pl.pallas_call(
        body,
        out_shape=outs,
        in_specs=[hbm if k in stay else vmem for k in range(len(args))],
        out_specs=jax.tree.map(lambda _: vmem, outs),
        scratch_shapes=scratch,
        compiler_params=pltpu.CompilerParams(vmem_limit_bytes=24 * 2**20),
        name=body.__name__,
    )(*placed)


def struct(shape, dtype):
    return pltpu.VMEM(shape, dtype)


def iota(shape, dim):
    return lax.broadcasted_iota(jnp.int32, shape, dim)


def dot(left, right):
    return jnp.dot(left, right, preferred_element_type=f32)


def rounded(value):
    return value.astype(bf16).astype(f32)


def as_row(column):
    rows = column.shape[0]
    seen = jnp.where(iota((rows, lanes), 0) == iota((rows, lanes), 1), column, 0.0)
    return jnp.sum(seen, axis=0, keepdims=True)


def as_column(row, rows):
    seen = jnp.where(iota((rows, lanes), 0) == iota((rows, lanes), 1), row, 0.0)
    return jnp.sum(seen, axis=1, keepdims=True)


def silu(value):
    return value * jax.nn.sigmoid(value)


def attend(
    tok_hbm,
    wq_hbm,
    dd_hbm,
    du_hbm,
    state_hbm,
    wk_hbm,
    wv_hbm,
    wg_hbm,
    wo_hbm,
    db_hbm,
    hg_hbm,
    out_ref,
    done_ref,
    tok_ref,
    wq_ref,
    dd_ref,
    du_ref,
    state_ref,
    wk_ref,
    wv_ref,
    wg_ref,
    wo_ref,
    db_ref,
    hg_ref,
    sems,
):
    rows = tok_ref.shape[0]
    key_dim = wq_ref.shape[1]
    parts = sems.shape[0] - 10
    step = rows // parts
    copies = [
        pltpu.make_async_copy(a, b, sems.at[k])
        for k, (a, b) in enumerate(
            (
                (tok_hbm, tok_ref),
                (wq_hbm, wq_ref),
                (dd_hbm, dd_ref),
                (du_hbm, du_ref),
                (db_hbm, db_ref),
                (hg_hbm, hg_ref),
            )
        )
    ]
    pieces = [
        pltpu.make_async_copy(
            state_hbm.at[pl.ds(p * step, step)], state_ref.at[pl.ds(p * step, step)], sems.at[10 + p]
        )
        for p in range(parts)
    ]
    later = [
        pltpu.make_async_copy(a, b, sems.at[6 + k])
        for k, (a, b) in enumerate(
            ((wk_hbm, wk_ref), (wv_hbm, wv_ref), (wg_hbm, wg_ref), (wo_hbm, wo_ref))
        )
    ]
    for copy in copies + pieces + later:
        copy.start()
    copies[0].wait()
    copies[2].wait()
    copies[3].wait()
    copies[4].wait()
    tok = tok_ref[...]
    low = lax.dot_general(
        tok, dd_ref[...], (((1,), (1,)), ((), ())), preferred_element_type=f32
    ).astype(bf16)
    pre = dot(low, du_ref[...]) + db_ref[...]
    log_decay = (jnp.minimum(pre, 0.0) - jnp.log1p(jnp.exp(-jnp.abs(pre)))) / decay_tau
    decay = jnp.exp(log_decay)
    copies[1].wait()
    queries = rounded(dot(tok, wq_ref[...])) * key_dim ** (-0.5)
    decayed = queries * decay
    turned = jnp.concatenate([decayed, jnp.zeros((lanes - rows, key_dim), f32)], axis=0).T
    carried = []
    for p in range(parts):
        pieces[p].wait()
        for b in range(p * step, (p + 1) * step):
            carried.append(
                jnp.sum(turned[:, b : b + 1] * state_ref[b, 0], axis=0, keepdims=True)
            )
    carried = jnp.concatenate(carried, axis=0)
    later[0].wait()
    keys = rounded(dot(tok, wk_ref[...]))
    later[1].wait()
    values = rounded(dot(tok, wv_ref[...]))
    later[2].wait()
    gate = rounded(dot(tok, wg_ref[...]))
    copies[5].wait()
    attended = carried + jnp.sum(queries * keys, axis=1, keepdims=True) * values
    inv_norm = lax.rsqrt(jnp.mean(attended * attended, axis=1, keepdims=True) + norm_eps)
    head_out = (attended * inv_norm * hg_ref[...] * silu(gate)).astype(bf16)
    later[3].wait()
    partial = rounded(dot(head_out, wo_ref[...]))
    row = as_row(jnp.sum(partial, axis=1, keepdims=True))
    high = rounded(row)
    middle = rounded(row - high)
    low = row - high - middle
    at = iota((8, lanes), 0)
    tail = jnp.where(at == 0, high, jnp.where(at == 1, middle, jnp.where(at == 2, low, 0.0)))
    for j in range(out_ref.shape[0]):
        out_ref[j] = jnp.concatenate(
            [partial[:, j * lanes : (j + 1) * lanes], tail], axis=0
        ).astype(bf16)
    done_ref[...] = tail


def place(
    ids_ref, weight_ref, tok_ref, behind, send_ref, high_ref, low_ref, perm_ref, back_ref, own_ref
):
    top, rows = ids_ref.shape
    slots = send_ref.shape[0]
    blocks = slots // (4 * capacity)

    def square(ref):
        wide = jnp.concatenate([ref[...].astype(f32), jnp.zeros((top, lanes - rows), f32)], axis=1)
        return jnp.concatenate([wide, jnp.zeros((lanes - top, lanes), f32)], axis=0)

    ids, weights = square(ids_ref), square(weight_ref)
    slot = iota((slots, lanes), 0)
    expert = jnp.where(iota((slots, lanes), 1) < rows, slot // capacity, -1).astype(f32)
    hit = jnp.zeros((slots, lanes), f32)
    for k in range(top):
        hit = jnp.where(ids[k : k + 1, :] == expert, 1.0, hit)
    earlier = (iota((lanes, lanes), 0) < iota((lanes, lanes), 1)).astype(bf16)
    rank = dot(hit.astype(bf16), earlier)
    send_ref[...] = jnp.where(rank == (slot % capacity).astype(f32), hit, 0.0).astype(bf16)
    ids, weights = ids.T, weights.T
    slot = iota((rows, slots), 1)
    expert = (slot // capacity).astype(f32)
    hit = jnp.zeros((rows, slots), f32)
    weight = jnp.zeros((rows, slots), f32)
    for k in range(top):
        same = ids[:rows, k : k + 1] == expert
        hit = jnp.where(same, 1.0, hit)
        weight = jnp.where(same, weights[:rows, k : k + 1], weight)
    earlier = (iota((rows, rows), 1) < iota((rows, rows), 0)).astype(bf16)
    rank = dot(earlier, hit.astype(bf16))
    weight = jnp.where(rank == (slot % capacity).astype(f32), weight, 0.0)
    high = weight.astype(bf16)
    high_ref[...] = high
    low_ref[...] = (weight - high.astype(f32)).astype(bf16)
    per_expert = blocks * capacity

    def source(at):
        expert, rest = at // per_expert, at % per_expert
        return rest // capacity * (4 * capacity) + expert * capacity + rest % capacity

    one, two = iota((slots, slots), 0), iota((slots, slots), 1)
    perm_ref[...] = (source(iota((slots, 1), 0)) == two).astype(bf16)
    back_ref[...] = (one == source(iota((1, slots), 1))).astype(bf16)
    width = tok_ref.shape[1]
    start = pl.multiple_of(lax.axis_index("tp") * lanes, lanes)
    mean = jnp.sum(tok_ref[...].astype(f32), axis=1, keepdims=True) / width
    own_ref[...] = res_scale * (tok_ref[:, pl.ds(start, lanes)].astype(f32) - mean)


def dispatch(got_ref, own_ref, gain_ref, send_ref, rows_ref, centred_ref, width):
    rows = own_ref.shape[0]
    total = jnp.sum(got_ref[...].astype(f32), axis=0)
    mixed = rounded(total[:rows])
    sums = total[rows : rows + 1] + total[rows + 1 : rows + 2] + total[rows + 2 : rows + 3]
    centred = own_ref[...] + mixed - as_column(sums, rows) / width
    centred_ref[...] = centred
    scaled = centred * gain_ref[...]
    filled = jnp.concatenate([scaled, jnp.zeros((lanes - rows, lanes), f32)], axis=0)
    rows_ref[...] = dot(send_ref[...], filled.astype(bf16)).astype(bf16)


def two_parts(column):
    high = rounded(column)
    return high, column - high


def expand(rows_ref, perm_ref, gate_ref, up_ref, sg_ref, su_ref, gain_ref, centred_ref, out_ref):
    chunks, rows, width = out_ref.shape
    experts, _, hidden = gate_ref.shape
    sorted_rows = dot(perm_ref[...], rows_ref[...])
    scale = sorted_rows / gain_ref[...]
    high, low = two_parts(jnp.sum(scale * scale, axis=1, keepdims=True))
    centred = centred_ref[...]
    own_high, own_low = two_parts(jnp.sum(centred * centred, axis=1, keepdims=True))
    own = (centred * gain_ref[...]).astype(bf16)
    shared_gate, shared_up = dot(own, sg_ref[...]), dot(own, su_ref[...])
    lane = iota((rows, lanes), 1)
    share = hidden // chunks
    per = chunks // experts
    for e in range(experts):
        taken = sorted_rows[e * per * rows : (e + 1) * per * rows].astype(bf16)
        gate, up = dot(taken, gate_ref[e]), dot(taken, up_ref[e])
        for q in range(per):
            j = e * per + q
            cut = slice(q * rows, (q + 1) * rows)
            out_ref[j, :, 0:hidden] = gate[cut].astype(bf16)
            out_ref[j, :, hidden : 2 * hidden] = up[cut].astype(bf16)
            tile = j * share // lanes * lanes
            turn = j * share % lanes
            g = pltpu.roll(shared_gate[:, tile : tile + lanes], (lanes - turn) % lanes, 1)
            u = pltpu.roll(shared_up[:, tile : tile + lanes], (lanes + share - turn) % lanes, 1)
            whole = slice(j * rows, (j + 1) * rows)
            last = jnp.where(lane < share, g, jnp.where(lane < 2 * share, u, 0.0))
            last = jnp.where(lane == 2 * share, high[whole], last)
            last = jnp.where(lane == 2 * share + 1, low[whole], last)
            last = jnp.where(lane == 2 * share + 2, own_high, last)
            last = jnp.where(lane == 2 * share + 3, own_low, last)
            out_ref[j, :, 2 * hidden :] = last.astype(bf16)


def activate(got_ref, inner_ref, own_ref, width):
    chunks, rows, _ = got_ref.shape
    hidden = inner_ref.shape[1] - lanes
    share = hidden // chunks
    total = jnp.sum(got_ref[...].astype(f32), axis=0)
    last = total[:, 2 * hidden :]

    def inv_std(at):
        squares = last[:, at : at + 1] + last[:, at + 1 : at + 2]
        return lax.rsqrt(squares / width + norm_eps)

    inv = inv_std(2 * share)
    gate = rounded(total[:, :hidden] * inv)
    up = rounded(total[:, hidden : 2 * hidden] * inv)
    inner_ref[:, :hidden] = (silu(gate) * up).astype(bf16)
    inv = inv_std(2 * share + 2)
    own_ref[...] = jnp.broadcast_to(inv, own_ref.shape)
    both = rounded(last * inv)
    up = pltpu.roll(both, lanes - share, 1)
    lane = iota((rows, lanes), 1)
    inner_ref[:, hidden:] = jnp.where(lane < share, silu(both) * up, 0.0).astype(bf16)


def contract(inner_ref, back_ref, down_ref, out_ref, done_ref):
    experts, hidden, _ = down_ref.shape
    per = inner_ref.shape[0] // experts
    outs = [
        dot(inner_ref[e * per : (e + 1) * per, :hidden], down_ref[e]).astype(bf16)
        for e in range(experts)
    ]
    out_ref[...] = dot(back_ref[...], jnp.concatenate(outs, axis=0)).astype(bf16)
    done_ref[...] = jnp.zeros(done_ref.shape, f32)


def share_out(inner_ref, down_ref, centred_ref, gain_ref, inv_ref, behind, base_ref):
    chunks, _, width = inner_ref.shape
    hidden = width - lanes
    share = hidden // chunks
    normed = rounded(centred_ref[...] * inv_ref[...] * gain_ref[...])
    total = res_scale * normed
    for j in range(chunks):
        total += dot(
            inner_ref[j, :, hidden : hidden + share], down_ref[j * share : (j + 1) * share]
        )
    base_ref[...] = total


def combine(got_ref, high_ref, low_ref, base_ref, resid_ref, stats_ref):
    got = got_ref[...]
    resid = base_ref[...] + dot(high_ref[...], got) + dot(low_ref[...], got)
    resid_ref[...] = resid
    sums = as_row(jnp.sum(resid, axis=1, keepdims=True))
    squares = as_row(jnp.sum(resid * resid, axis=1, keepdims=True))
    at = iota((8, lanes), 0)
    tile = jnp.where(at == 0, sums, jnp.where(at == 1, squares, 0.0))
    for j in range(stats_ref.shape[0]):
        stats_ref[j] = tile


def finish(got_ref, resid_ref, gain_ref, out_ref, width):
    rows = resid_ref.shape[0]
    total = jnp.sum(got_ref[...], axis=0)
    mean = as_column(total[0:1], rows) / width
    spread = as_column(total[1:2], rows) / width - mean * mean
    out_ref[...] = (
        (resid_ref[...] - mean) * lax.rsqrt(spread + norm_eps) * gain_ref[...]
    ).astype(bf16)


def to_each(value, axis):
    return lax.all_to_all(value, axis, split_axis=0, concat_axis=0, tiled=True)


def per_device(
    tokens,
    state,
    w_query,
    w_key,
    w_value,
    w_outgate,
    decay_down,
    decay_up,
    decay_bias,
    head_gain,
    w_output,
    norm1_gain,
    route_ids,
    route_weight,
    exp_gate,
    exp_up,
    exp_down,
    sh_gate,
    sh_up,
    sh_down,
    norm2_gain,
):
    rows, width = tokens.shape
    tp_count, ep_count = lax.axis_size("tp"), lax.axis_size("ep")
    cols = width // tp_count
    hidden = exp_gate.shape[2]
    per_block = exp_gate.shape[0] * capacity
    slots = ep_count * per_block
    gain1, gain2 = norm1_gain.reshape(1, cols), norm2_gain.reshape(1, cols)

    held = (
        tokens,
        w_query,
        decay_down.T,
        decay_up,
        state,
        w_key,
        w_value,
        w_outgate,
        w_output,
        decay_bias.reshape(1, -1),
        head_gain.reshape(1, -1),
    )
    outgoing, done = local_call(
        attend,
        (struct((tp_count, rows + 8, cols), bf16), struct((8, cols), f32)),
        held,
        stay=tuple(range(len(held))),
        scratch=[pltpu.VMEM(a.shape, a.dtype) for a in held] + [pltpu.SemaphoreType.DMA((13,))],
    )
    arrived = to_each(outgoing, "tp")
    send, high, low, perm, back, own = local_call(
        place,
        (
            struct((slots, lanes), bf16),
            struct((rows, slots), bf16),
            struct((rows, slots), bf16),
            struct((slots, slots), bf16),
            struct((slots, slots), bf16),
            struct((rows, cols), f32),
        ),
        (route_ids.T, route_weight.T, tokens, done),
    )

    def named(body):
        def call(*refs):
            body(*refs, width)

        call.__name__ = body.__name__
        return call

    sent, centred = local_call(
        named(dispatch),
        (struct((slots, cols), bf16), struct((rows, cols), f32)),
        (arrived, own, gain1, send),
    )
    taken = to_each(sent.reshape(ep_count, per_block, cols), "ep").reshape(slots, cols)
    partials = local_call(
        expand,
        struct((tp_count, rows, 2 * hidden + lanes), bf16),
        (taken, perm, exp_gate, exp_up, sh_gate, sh_up, gain1, centred),
    )
    parts = to_each(partials, "tp")

    inner, inv = local_call(
        named(activate),
        (struct((rows, hidden + lanes), bf16), struct((rows, cols), f32)),
        (parts,),
    )
    inners = lax.all_gather(inner, "tp", axis=0, tiled=True)
    result, done = local_call(
        contract,
        (struct((slots, cols), bf16), struct((8, cols), f32)),
        (inners, back, exp_down),
    )
    returned = to_each(result.reshape(ep_count, per_block, cols), "ep").reshape(slots, cols)
    base = local_call(
        share_out,
        struct((rows, cols), f32),
        (inners.reshape(tp_count, rows, -1), sh_down, centred, gain1, inv, done),
    )
    resid, stats = local_call(
        combine,
        (struct((rows, cols), f32), struct((tp_count, 8, lanes), f32)),
        (returned, high, low, base),
    )
    all_stats = to_each(stats, "tp")

    return local_call(
        named(finish), jax.ShapeDtypeStruct((rows, cols), bf16), (all_stats, resid, gain2)
    )


def solution(mesh):
    in_specs = (
        P("ep", None),
        P("ep", "tp", None, None),
        P(None, "tp"),
        P(None, "tp"),
        P(None, "tp"),
        P(None, "tp"),
        P(),
        P(None, "tp"),
        P("tp"),
        P(),
        P("tp", None),
        P("tp"),
        P("ep", None),
        P("ep", None),
        P("ep", "tp", None),
        P("ep", "tp", None),
        P("ep", None, "tp"),
        P("tp", None),
        P("tp", None),
        P(None, "tp"),
        P("tp"),
    )
    out_specs = P("ep", "tp")
    return jax.shard_map(
        per_device, mesh=mesh, in_specs=in_specs, out_specs=out_specs, check_vma=False
    )
```

```python
import jax
import jax.numpy as jnp
from jax import lax
from jax.experimental import pallas as pl
from jax.experimental.pallas import tpu as pltpu
from jax.sharding import PartitionSpec as P

res_scale = 2.0**0.5
decay_tau = 16.0
norm_eps = 1e-05
capacity = 2
lanes = 128

f32 = jnp.float32
bf16 = jnp.bfloat16


def local_call(body, outs, args, stay=(), scratch=()):
    vmem = pl.BlockSpec(memory_space=pltpu.VMEM)
    hbm = pl.BlockSpec(memory_space=pl.ANY)
    placed = [
        pltpu.with_memory_space_constraint(a, pltpu.HBM if k in stay else pltpu.VMEM)
        for k, a in enumerate(args)
    ]
    return pl.pallas_call(
        body,
        out_shape=outs,
        in_specs=[hbm if k in stay else vmem for k in range(len(args))],
        out_specs=jax.tree.map(lambda _: vmem, outs),
        scratch_shapes=scratch,
        compiler_params=pltpu.CompilerParams(vmem_limit_bytes=24 * 2**20),
        name=body.__name__,
    )(*placed)


def struct(shape, dtype):
    return pltpu.VMEM(shape, dtype)


def iota(shape, dim):
    return lax.broadcasted_iota(jnp.int32, shape, dim)


def dot(left, right):
    return jnp.dot(left, right, preferred_element_type=f32)


def rounded(value):
    return value.astype(bf16).astype(f32)


def as_row(column):
    rows = column.shape[0]
    seen = jnp.where(iota((rows, lanes), 0) == iota((rows, lanes), 1), column, 0.0)
    return jnp.sum(seen, axis=0, keepdims=True)


def as_column(row, rows):
    seen = jnp.where(iota((rows, lanes), 0) == iota((rows, lanes), 1), row, 0.0)
    return jnp.sum(seen, axis=1, keepdims=True)


def silu(value):
    return value * jax.nn.sigmoid(value)


def route(ids_ref, weight_ref, send_ref, high_ref, low_ref, perm_ref, back_ref):
    top, rows = ids_ref.shape
    slots = send_ref.shape[0]
    blocks = slots // (4 * capacity)

    def square(ref):
        wide = jnp.concatenate([ref[...].astype(f32), jnp.zeros((top, lanes - rows), f32)], axis=1)
        return jnp.concatenate([wide, jnp.zeros((lanes - top, lanes), f32)], axis=0)

    ids, weights = square(ids_ref), square(weight_ref)
    slot = iota((slots, lanes), 0)
    expert = jnp.where(iota((slots, lanes), 1) < rows, slot // capacity, -1).astype(f32)
    hit = jnp.zeros((slots, lanes), f32)
    for k in range(top):
        hit = jnp.where(ids[k : k + 1, :] == expert, 1.0, hit)
    earlier = (iota((lanes, lanes), 0) < iota((lanes, lanes), 1)).astype(bf16)
    rank = dot(hit.astype(bf16), earlier)
    send_ref[...] = jnp.where(rank == (slot % capacity).astype(f32), hit, 0.0).astype(bf16)
    ids, weights = ids.T, weights.T
    slot = iota((rows, slots), 1)
    expert = (slot // capacity).astype(f32)
    hit = jnp.zeros((rows, slots), f32)
    weight = jnp.zeros((rows, slots), f32)
    for k in range(top):
        same = ids[:rows, k : k + 1] == expert
        hit = jnp.where(same, 1.0, hit)
        weight = jnp.where(same, weights[:rows, k : k + 1], weight)
    earlier = (iota((rows, rows), 1) < iota((rows, rows), 0)).astype(bf16)
    rank = dot(earlier, hit.astype(bf16))
    weight = jnp.where(rank == (slot % capacity).astype(f32), weight, 0.0)
    high = weight.astype(bf16)
    high_ref[...] = high
    low_ref[...] = (weight - high.astype(f32)).astype(bf16)
    per_expert = blocks * capacity

    def source(at):
        expert, rest = at // per_expert, at % per_expert
        return rest // capacity * (4 * capacity) + expert * capacity + rest % capacity

    one, two = iota((slots, slots), 0), iota((slots, slots), 1)
    perm_ref[...] = (source(iota((slots, 1), 0)) == two).astype(bf16)
    back_ref[...] = (one == source(iota((1, slots), 1))).astype(bf16)


def attend(*refs):
    count = 13
    far, out_ref, tables, own_ref = refs[:count], refs[count], refs[count + 1 : count + 6], refs[count + 6]
    near, sems = refs[count + 7 : -1], refs[-1]
    ids, weights, tok, dd, du, db, wq, wk, wv, wg, hg, state, wo = range(count)
    copies = [pltpu.make_async_copy(a, b, sems.at[k]) for k, (a, b) in enumerate(zip(far, near))]
    for copy in copies:
        copy.start()

    def ready(*which):
        for k in which:
            copies[k].wait()

    ready(ids, weights)
    route(near[ids], near[weights], *tables)
    ready(tok, dd, du, db)
    tok_ref = near[tok]
    rows, width = tok_ref.shape
    tokens = tok_ref[...]
    start = pl.multiple_of(lax.axis_index("tp") * lanes, lanes)
    mean = jnp.sum(tokens.astype(f32), axis=1, keepdims=True) / width
    own_ref[...] = res_scale * (tok_ref[:, pl.ds(start, lanes)].astype(f32) - mean)
    low = lax.dot_general(
        tokens, near[dd][...], (((1,), (1,)), ((), ())), preferred_element_type=f32
    ).astype(bf16)
    pre = dot(low, near[du][...]) + near[db][...]
    log_decay = (jnp.minimum(pre, 0.0) - jnp.log1p(jnp.exp(-jnp.abs(pre)))) / decay_tau
    decay = jnp.exp(log_decay)
    ready(wq)
    key_dim = near[wq].shape[1]
    queries = rounded(dot(tokens, near[wq][...])) * key_dim ** (-0.5)
    decayed = queries * decay
    turned = jnp.concatenate([decayed, jnp.zeros((lanes - rows, key_dim), f32)], axis=0).T
    ready(wk, wv)
    keys = rounded(dot(tokens, near[wk][...]))
    values = rounded(dot(tokens, near[wv][...]))
    ready(wg, hg, state)
    gate = rounded(dot(tokens, near[wg][...]))
    carried = jnp.concatenate(
        [
            jnp.sum(turned[:, b : b + 1] * near[state][b, 0], axis=0, keepdims=True)
            for b in range(rows)
        ],
        axis=0,
    )
    attended = carried + jnp.sum(queries * keys, axis=1, keepdims=True) * values
    inv_norm = lax.rsqrt(jnp.mean(attended * attended, axis=1, keepdims=True) + norm_eps)
    head_out = (attended * inv_norm * near[hg][...] * silu(gate)).astype(bf16)
    ready(wo)
    partial = rounded(dot(head_out, near[wo][...]))
    row = as_row(jnp.sum(partial, axis=1, keepdims=True))
    high = rounded(row)
    middle = rounded(row - high)
    low = row - high - middle
    at = iota((8, lanes), 0)
    tail = jnp.where(at == 0, high, jnp.where(at == 1, middle, jnp.where(at == 2, low, 0.0)))
    for j in range(out_ref.shape[0]):
        out_ref[j] = jnp.concatenate(
            [partial[:, j * lanes : (j + 1) * lanes], tail], axis=0
        ).astype(bf16)


def dispatch(got_ref, own_ref, gain_ref, send_ref, rows_ref, centred_ref, width):
    rows = own_ref.shape[0]
    total = jnp.sum(got_ref[...].astype(f32), axis=0)
    mixed = rounded(total[:rows])
    sums = total[rows : rows + 1] + total[rows + 1 : rows + 2] + total[rows + 2 : rows + 3]
    centred = own_ref[...] + mixed - as_column(sums, rows) / width
    centred_ref[...] = centred
    scaled = centred * gain_ref[...]
    filled = jnp.concatenate([scaled, jnp.zeros((lanes - rows, lanes), f32)], axis=0)
    rows_ref[...] = dot(send_ref[...], filled.astype(bf16)).astype(bf16)


def two_parts(column):
    high = rounded(column)
    return high, column - high


def expand(
    rows_ref, perm_ref, gate_ref, up_ref, sg_ref, su_ref, gain_ref, centred_ref, keep_ref, send_ref
):
    pairs, rows, _ = keep_ref.shape
    experts, _, hidden = gate_ref.shape
    chunks = 2 * pairs
    even = lax.rem(lax.axis_index("tp"), 2) == 0
    sorted_rows = dot(perm_ref[...], rows_ref[...])
    scale = sorted_rows / gain_ref[...]
    high, low = two_parts(jnp.sum(scale * scale, axis=1, keepdims=True))
    centred = centred_ref[...]
    own_high, own_low = two_parts(jnp.sum(centred * centred, axis=1, keepdims=True))
    own = (centred * gain_ref[...]).astype(bf16)
    shared_gate, shared_up = dot(own, sg_ref[...]), dot(own, su_ref[...])
    lane = iota((rows, lanes), 1)
    share = hidden // chunks
    per = chunks // experts

    def last_block(j):
        tile = j * share // lanes * lanes
        turn = j * share % lanes
        g = pltpu.roll(shared_gate[:, tile : tile + lanes], (lanes - turn) % lanes, 1)
        u = pltpu.roll(shared_up[:, tile : tile + lanes], (lanes + share - turn) % lanes, 1)
        whole = slice(j * rows, (j + 1) * rows)
        last = jnp.where(lane < share, g, jnp.where(lane < 2 * share, u, 0.0))
        last = jnp.where(lane == 2 * share, high[whole], last)
        last = jnp.where(lane == 2 * share + 1, low[whole], last)
        last = jnp.where(lane == 2 * share + 2, own_high, last)
        return jnp.where(lane == 2 * share + 3, own_low, last)

    for e in range(experts):
        taken = sorted_rows[e * per * rows : (e + 1) * per * rows].astype(bf16)
        gate, up = dot(taken, gate_ref[e]), dot(taken, up_ref[e])
        for q in range(0, per, 2):
            j = e * per + q
            one, two = slice(q * rows, (q + 1) * rows), slice((q + 1) * rows, (q + 2) * rows)
            for at, a, b in (
                (slice(0, hidden), gate[one], gate[two]),
                (slice(hidden, 2 * hidden), up[one], up[two]),
                (slice(2 * hidden, 2 * hidden + lanes), last_block(j), last_block(j + 1)),
            ):
                keep_ref[j // 2, :, at] = jnp.where(even, a, b).astype(bf16)
                send_ref[j // 2, :, at] = jnp.where(even, b, a).astype(bf16)


def pair(keep_ref, got_ref, out_ref):
    pairs, rows, width = keep_ref.shape
    total = keep_ref[...].astype(f32) + got_ref[...].astype(f32)
    wide = width - lanes
    out_ref[:, :, :wide] = total[:, :, :wide].astype(bf16)
    last = total[:, :, wide:]
    lane = iota(last.shape, 2)
    share = wide // 2 // (2 * pairs)
    for at in (2 * share, 2 * share + 2):
        high, low = two_parts(last[:, :, at : at + 1] + last[:, :, at + 1 : at + 2])
        last = jnp.where(lane == at, high, jnp.where(lane == at + 1, low, last))
    out_ref[:, :, wide:] = last.astype(bf16)


def activate(got_ref, inner_ref, own_ref, width):
    rows = got_ref.shape[1]
    chunks = 2 * got_ref.shape[0]
    hidden = inner_ref.shape[1] - lanes
    share = hidden // chunks
    total = jnp.sum(got_ref[...].astype(f32), axis=0)
    last = total[:, 2 * hidden :]

    def inv_std(at):
        squares = last[:, at : at + 1] + last[:, at + 1 : at + 2]
        return lax.rsqrt(squares / width + norm_eps)

    inv = inv_std(2 * share)
    gate = rounded(total[:, :hidden] * inv)
    up = rounded(total[:, hidden : 2 * hidden] * inv)
    inner_ref[:, :hidden] = (silu(gate) * up).astype(bf16)
    inv = inv_std(2 * share + 2)
    own_ref[...] = jnp.broadcast_to(inv, own_ref.shape)
    both = rounded(last * inv)
    up = pltpu.roll(both, lanes - share, 1)
    lane = iota((rows, lanes), 1)
    inner_ref[:, hidden:] = jnp.where(lane < share, silu(both) * up, 0.0).astype(bf16)


def contract(inner_ref, back_ref, down_ref, shared_ref, centred_ref, gain_ref, inv_ref, out_ref, base_ref):
    experts, hidden, _ = down_ref.shape
    chunks, rows, _ = inner_ref.shape
    per = chunks // experts
    share = hidden // chunks
    outs = []
    for e in range(experts):
        inner = jnp.concatenate(
            [inner_ref[j, :, :hidden].astype(f32) for j in range(e * per, (e + 1) * per)], axis=0
        )
        outs.append(dot(inner.astype(bf16), down_ref[e]).astype(bf16))
    out_ref[...] = dot(back_ref[...], jnp.concatenate(outs, axis=0)).astype(bf16)
    normed = rounded(centred_ref[...] * inv_ref[...] * gain_ref[...])
    lane = iota((rows, lanes), 1)
    tiles = []
    for t in range(hidden // lanes):
        tile = jnp.zeros((rows, lanes), f32)
        for k in range(lanes // share):
            piece = inner_ref[t * (lanes // share) + k, :, hidden:].astype(f32)
            tile = jnp.where(lane // share == k, pltpu.roll(piece, k * share, 1), tile)
        tiles.append(tile)
    shared = jnp.concatenate(tiles, axis=1).astype(bf16)
    base_ref[...] = res_scale * normed + dot(shared, shared_ref[...])


def combine(got_ref, high_ref, low_ref, base_ref, resid_ref, stats_ref):
    got = got_ref[...]
    resid = base_ref[...] + dot(high_ref[...], got) + dot(low_ref[...], got)
    resid_ref[...] = resid
    sums = as_row(jnp.sum(resid, axis=1, keepdims=True))
    squares = as_row(jnp.sum(resid * resid, axis=1, keepdims=True))
    at = iota((8, lanes), 0)
    tile = jnp.where(at == 0, sums, jnp.where(at == 1, squares, 0.0))
    for j in range(stats_ref.shape[0]):
        stats_ref[j] = tile


def finish(got_ref, resid_ref, gain_ref, out_ref, width):
    rows = resid_ref.shape[0]
    total = jnp.sum(got_ref[...], axis=0)
    mean = as_column(total[0:1], rows) / width
    spread = as_column(total[1:2], rows) / width - mean * mean
    out_ref[...] = (
        (resid_ref[...] - mean) * lax.rsqrt(spread + norm_eps) * gain_ref[...]
    ).astype(bf16)


def to_each(value, axis):
    return lax.all_to_all(value, axis, split_axis=0, concat_axis=0, tiled=True)


def per_device(
    tokens,
    state,
    w_query,
    w_key,
    w_value,
    w_outgate,
    decay_down,
    decay_up,
    decay_bias,
    head_gain,
    w_output,
    norm1_gain,
    route_ids,
    route_weight,
    exp_gate,
    exp_up,
    exp_down,
    sh_gate,
    sh_up,
    sh_down,
    norm2_gain,
):
    rows, width = tokens.shape
    tp_count, ep_count = lax.axis_size("tp"), lax.axis_size("ep")
    cols = width // tp_count
    hidden = exp_gate.shape[2]
    per_block = exp_gate.shape[0] * capacity
    slots = ep_count * per_block
    gain1, gain2 = norm1_gain.reshape(1, cols), norm2_gain.reshape(1, cols)

    held = (
        route_ids.T,
        route_weight.T,
        tokens,
        decay_down.T,
        decay_up,
        decay_bias.reshape(1, -1),
        w_query,
        w_key,
        w_value,
        w_outgate,
        head_gain.reshape(1, -1),
        state,
        w_output,
    )
    outgoing, send, high, low, perm, back, own = local_call(
        attend,
        (
            struct((tp_count, rows + 8, cols), bf16),
            struct((slots, lanes), bf16),
            struct((rows, slots), bf16),
            struct((rows, slots), bf16),
            struct((slots, slots), bf16),
            struct((slots, slots), bf16),
            struct((rows, cols), f32),
        ),
        held,
        stay=tuple(range(len(held))),
        scratch=[pltpu.VMEM(a.shape, a.dtype) for a in held]
        + [pltpu.SemaphoreType.DMA((len(held),))],
    )
    arrived = to_each(outgoing, "tp")

    def named(body):
        def call(*refs):
            body(*refs, width)

        call.__name__ = body.__name__
        return call

    sent, centred = local_call(
        named(dispatch),
        (struct((slots, cols), bf16), struct((rows, cols), f32)),
        (arrived, own, gain1, send),
    )
    taken = to_each(sent.reshape(ep_count, per_block, cols), "ep").reshape(slots, cols)
    block = struct((tp_count // 2, rows, 2 * hidden + lanes), bf16)
    keep, give = local_call(
        expand,
        (block, block),
        (taken, perm, exp_gate, exp_up, sh_gate, sh_up, gain1, centred),
    )
    other = lax.ppermute(give, "tp", [(i, i ^ 1) for i in range(tp_count)])
    partials = local_call(pair, block, (keep, other))
    same_core = [list(range(core, tp_count, 2)) for core in range(2)]
    parts = lax.all_to_all(partials, "tp", 0, 0, tiled=True, axis_index_groups=same_core)
    inner, inv = local_call(
        named(activate),
        (struct((rows, hidden + lanes), bf16), struct((rows, cols), f32)),
        (parts,),
    )
    inners = lax.all_gather(inner, "tp", axis=0)
    result, base = local_call(
        contract,
        (struct((slots, cols), bf16), struct((rows, cols), f32)),
        (inners, back, exp_down, sh_down, centred, gain1, inv),
    )
    returned = to_each(result.reshape(ep_count, per_block, cols), "ep").reshape(slots, cols)
    resid, stats = local_call(
        combine,
        (struct((rows, cols), f32), struct((tp_count, 8, lanes), f32)),
        (returned, high, low, base),
    )
    all_stats = to_each(stats, "tp")

    return local_call(
        named(finish), jax.ShapeDtypeStruct((rows, cols), bf16), (all_stats, resid, gain2)
    )


def solution(mesh):
    in_specs = (
        P("ep", None),
        P("ep", "tp", None, None),
        P(None, "tp"),
        P(None, "tp"),
        P(None, "tp"),
        P(None, "tp"),
        P(),
        P(None, "tp"),
        P("tp"),
        P(),
        P("tp", None),
        P("tp"),
        P("ep", None),
        P("ep", None),
        P("ep", "tp", None),
        P("ep", "tp", None),
        P("ep", None, "tp"),
        P("tp", None),
        P("tp", None),
        P(None, "tp"),
        P("tp"),
    )
    out_specs = P("ep", "tp")
    return jax.shard_map(
        per_device, mesh=mesh, in_specs=in_specs, out_specs=out_specs, check_vma=False
    )
```

```python
import jax
import jax.numpy as jnp
from jax import lax
from jax.experimental import pallas as pl
from jax.experimental.pallas import tpu as pltpu
from jax.sharding import PartitionSpec as P

res_scale = 2.0**0.5
decay_tau = 16.0
norm_eps = 1e-05
capacity = 2
lanes = 128

f32 = jnp.float32
bf16 = jnp.bfloat16


def local_call(body, outs, args, stay=(), scratch=()):
    vmem = pl.BlockSpec(memory_space=pltpu.VMEM)
    hbm = pl.BlockSpec(memory_space=pl.ANY)
    placed = [
        pltpu.with_memory_space_constraint(a, pltpu.HBM if k in stay else pltpu.VMEM)
        for k, a in enumerate(args)
    ]
    return pl.pallas_call(
        body,
        out_shape=outs,
        in_specs=[hbm if k in stay else vmem for k in range(len(args))],
        out_specs=jax.tree.map(lambda _: vmem, outs),
        scratch_shapes=scratch,
        compiler_params=pltpu.CompilerParams(vmem_limit_bytes=24 * 2**20),
        name=body.__name__,
    )(*placed)


def struct(shape, dtype):
    return pltpu.VMEM(shape, dtype)


def iota(shape, dim):
    return lax.broadcasted_iota(jnp.int32, shape, dim)


def dot(left, right):
    return jnp.dot(left, right, preferred_element_type=f32)


def rounded(value):
    return value.astype(bf16).astype(f32)


def as_row(column):
    rows = column.shape[0]
    seen = jnp.where(iota((rows, lanes), 0) == iota((rows, lanes), 1), column, 0.0)
    return jnp.sum(seen, axis=0, keepdims=True)


def as_column(row, rows):
    seen = jnp.where(iota((rows, lanes), 0) == iota((rows, lanes), 1), row, 0.0)
    return jnp.sum(seen, axis=1, keepdims=True)


def silu(value):
    return value * jax.nn.sigmoid(value)


def route(ids_ref, weight_ref, send_ref, high_ref, low_ref, perm_ref, back_ref):
    top, rows = ids_ref.shape
    slots = send_ref.shape[0]
    blocks = slots // (4 * capacity)

    def square(ref):
        wide = jnp.concatenate([ref[...].astype(f32), jnp.zeros((top, lanes - rows), f32)], axis=1)
        return jnp.concatenate([wide, jnp.zeros((lanes - top, lanes), f32)], axis=0)

    ids, weights = square(ids_ref), square(weight_ref)
    slot = iota((slots, lanes), 0)
    expert = jnp.where(iota((slots, lanes), 1) < rows, slot // capacity, -1).astype(f32)
    hit = jnp.zeros((slots, lanes), f32)
    for k in range(top):
        hit = jnp.where(ids[k : k + 1, :] == expert, 1.0, hit)
    earlier = (iota((lanes, lanes), 0) < iota((lanes, lanes), 1)).astype(bf16)
    rank = dot(hit.astype(bf16), earlier)
    send_ref[...] = jnp.where(rank == (slot % capacity).astype(f32), hit, 0.0).astype(bf16)
    ids, weights = ids.T, weights.T
    slot = iota((rows, slots), 1)
    expert = (slot // capacity).astype(f32)
    hit = jnp.zeros((rows, slots), f32)
    weight = jnp.zeros((rows, slots), f32)
    for k in range(top):
        same = ids[:rows, k : k + 1] == expert
        hit = jnp.where(same, 1.0, hit)
        weight = jnp.where(same, weights[:rows, k : k + 1], weight)
    earlier = (iota((rows, rows), 1) < iota((rows, rows), 0)).astype(bf16)
    rank = dot(earlier, hit.astype(bf16))
    weight = jnp.where(rank == (slot % capacity).astype(f32), weight, 0.0)
    high = weight.astype(bf16)
    high_ref[...] = high
    low_ref[...] = (weight - high.astype(f32)).astype(bf16)
    per_expert = blocks * capacity

    def source(at):
        expert, rest = at // per_expert, at % per_expert
        return rest // capacity * (4 * capacity) + expert * capacity + rest % capacity

    one, two = iota((slots, slots), 0), iota((slots, slots), 1)
    perm_ref[...] = (source(iota((slots, 1), 0)) == two).astype(bf16)
    back_ref[...] = (one == source(iota((1, slots), 1))).astype(bf16)


def attend(*refs):
    count = 13
    far, out_ref, tables, own_ref = refs[:count], refs[count], refs[count + 1 : count + 6], refs[count + 6]
    near, sems = refs[count + 7 : -1], refs[-1]
    ids, weights, tok, dd, du, db, wq, wk, wv, wg, hg, state, wo = range(count)
    copies = [pltpu.make_async_copy(a, b, sems.at[k]) for k, (a, b) in enumerate(zip(far, near))]
    for copy in copies:
        copy.start()

    def ready(*which):
        for k in which:
            copies[k].wait()

    ready(ids, weights)
    route(near[ids], near[weights], *tables)
    ready(tok, dd, du, db)
    tok_ref = near[tok]
    rows, width = tok_ref.shape
    tokens = tok_ref[...]
    start = pl.multiple_of(lax.axis_index("tp") * lanes, lanes)
    mean = jnp.sum(tokens.astype(f32), axis=1, keepdims=True) / width
    own_ref[...] = res_scale * (tok_ref[:, pl.ds(start, lanes)].astype(f32) - mean)
    low = lax.dot_general(
        tokens, near[dd][...], (((1,), (1,)), ((), ())), preferred_element_type=f32
    ).astype(bf16)
    pre = dot(low, near[du][...]) + near[db][...]
    log_decay = (jnp.minimum(pre, 0.0) - jnp.log1p(jnp.exp(-jnp.abs(pre)))) / decay_tau
    decay = jnp.exp(log_decay)
    ready(wq)
    key_dim = near[wq].shape[1]
    queries = rounded(dot(tokens, near[wq][...])) * key_dim ** (-0.5)
    decayed = queries * decay
    turned = jnp.concatenate([decayed, jnp.zeros((lanes - rows, key_dim), f32)], axis=0).T
    ready(wk, wv)
    keys = rounded(dot(tokens, near[wk][...]))
    values = rounded(dot(tokens, near[wv][...]))
    ready(wg, hg, state)
    gate = rounded(dot(tokens, near[wg][...]))
    carried = jnp.concatenate(
        [
            jnp.sum(turned[:, b : b + 1] * near[state][b, 0], axis=0, keepdims=True)
            for b in range(rows)
        ],
        axis=0,
    )
    attended = carried + jnp.sum(queries * keys, axis=1, keepdims=True) * values
    inv_norm = lax.rsqrt(jnp.mean(attended * attended, axis=1, keepdims=True) + norm_eps)
    head_out = (attended * inv_norm * near[hg][...] * silu(gate)).astype(bf16)
    ready(wo)
    partial = rounded(dot(head_out, near[wo][...]))
    row = as_row(jnp.sum(partial, axis=1, keepdims=True))
    high = rounded(row)
    middle = rounded(row - high)
    low = row - high - middle
    at = iota((8, lanes), 0)
    tail = jnp.where(at == 0, high, jnp.where(at == 1, middle, jnp.where(at == 2, low, 0.0)))
    for j in range(out_ref.shape[0]):
        out_ref[j] = jnp.concatenate(
            [partial[:, j * lanes : (j + 1) * lanes], tail], axis=0
        ).astype(bf16)


def dispatch(got_ref, own_ref, gain_ref, send_ref, rows_ref, centred_ref, width):
    rows = own_ref.shape[0]
    total = jnp.sum(got_ref[...].astype(f32), axis=0)
    mixed = rounded(total[:rows])
    sums = total[rows : rows + 1] + total[rows + 1 : rows + 2] + total[rows + 2 : rows + 3]
    centred = own_ref[...] + mixed - as_column(sums, rows) / width
    centred_ref[...] = centred
    scaled = centred * gain_ref[...]
    filled = jnp.concatenate([scaled, jnp.zeros((lanes - rows, lanes), f32)], axis=0)
    rows_ref[...] = dot(send_ref[...], filled.astype(bf16)).astype(bf16)


def two_parts(column):
    high = rounded(column)
    return high, column - high


def expand(
    rows_ref, perm_ref, gate_ref, up_ref, sg_ref, su_ref, gain_ref, centred_ref, keep_ref, send_ref
):
    pairs, rows, _ = keep_ref.shape
    experts, _, hidden = gate_ref.shape
    chunks = 2 * pairs
    even = lax.rem(lax.axis_index("tp"), 2) == 0
    sorted_rows = dot(perm_ref[...], rows_ref[...])
    scale = sorted_rows / gain_ref[...]
    high, low = two_parts(jnp.sum(scale * scale, axis=1, keepdims=True))
    centred = centred_ref[...]
    own_high, own_low = two_parts(jnp.sum(centred * centred, axis=1, keepdims=True))
    own = (centred * gain_ref[...]).astype(bf16)
    shared_gate, shared_up = dot(own, sg_ref[...]), dot(own, su_ref[...])
    lane = iota((rows, lanes), 1)
    share = hidden // chunks
    per = chunks // experts

    def last_block(j):
        tile = j * share // lanes * lanes
        turn = j * share % lanes
        g = pltpu.roll(shared_gate[:, tile : tile + lanes], (lanes - turn) % lanes, 1)
        u = pltpu.roll(shared_up[:, tile : tile + lanes], (lanes + share - turn) % lanes, 1)
        whole = slice(j * rows, (j + 1) * rows)
        last = jnp.where(lane < share, g, jnp.where(lane < 2 * share, u, 0.0))
        last = jnp.where(lane == 2 * share, high[whole], last)
        last = jnp.where(lane == 2 * share + 1, low[whole], last)
        last = jnp.where(lane == 2 * share + 2, own_high, last)
        return jnp.where(lane == 2 * share + 3, own_low, last)

    for e in range(experts):
        taken = sorted_rows[e * per * rows : (e + 1) * per * rows].astype(bf16)
        gate, up = dot(taken, gate_ref[e]), dot(taken, up_ref[e])
        for q in range(0, per, 2):
            j = e * per + q
            one, two = slice(q * rows, (q + 1) * rows), slice((q + 1) * rows, (q + 2) * rows)
            for at, a, b in (
                (slice(0, hidden), gate[one], gate[two]),
                (slice(hidden, 2 * hidden), up[one], up[two]),
                (slice(2 * hidden, 2 * hidden + lanes), last_block(j), last_block(j + 1)),
            ):
                keep_ref[j // 2, :, at] = jnp.where(even, a, b).astype(bf16)
                send_ref[j // 2, :, at] = jnp.where(even, b, a).astype(bf16)


def pair(keep_ref, got_ref, out_ref):
    pairs, rows, width = keep_ref.shape
    total = keep_ref[...].astype(f32) + got_ref[...].astype(f32)
    wide = width - lanes
    out_ref[:, :, :wide] = total[:, :, :wide].astype(bf16)
    last = total[:, :, wide:]
    lane = iota(last.shape, 2)
    share = wide // 2 // (2 * pairs)
    for at in (2 * share, 2 * share + 2):
        high, low = two_parts(last[:, :, at : at + 1] + last[:, :, at + 1 : at + 2])
        last = jnp.where(lane == at, high, jnp.where(lane == at + 1, low, last))
    out_ref[:, :, wide:] = last.astype(bf16)


def activate(got_ref, inner_ref, own_ref, width):
    rows = got_ref.shape[1]
    chunks = 2 * got_ref.shape[0]
    hidden = inner_ref.shape[1] - lanes
    share = hidden // chunks
    total = jnp.sum(got_ref[...].astype(f32), axis=0)
    last = total[:, 2 * hidden :]

    def inv_std(at):
        squares = last[:, at : at + 1] + last[:, at + 1 : at + 2]
        return lax.rsqrt(squares / width + norm_eps)

    inv = inv_std(2 * share)
    gate = rounded(total[:, :hidden] * inv)
    up = rounded(total[:, hidden : 2 * hidden] * inv)
    inner_ref[:, :hidden] = (silu(gate) * up).astype(bf16)
    inv = inv_std(2 * share + 2)
    own_ref[...] = jnp.broadcast_to(inv, own_ref.shape)
    both = rounded(last * inv)
    up = pltpu.roll(both, lanes - share, 1)
    lane = iota((rows, lanes), 1)
    inner_ref[:, hidden:] = jnp.where(lane < share, silu(both) * up, 0.0).astype(bf16)


def contract(inner_ref, back_ref, down_ref, shared_ref, centred_ref, gain_ref, inv_ref, out_ref, base_ref):
    experts, hidden, _ = down_ref.shape
    chunks, rows, _ = inner_ref.shape
    per = chunks // experts
    share = hidden // chunks
    outs = []
    for e in range(experts):
        inner = jnp.concatenate(
            [inner_ref[j, :, :hidden].astype(f32) for j in range(e * per, (e + 1) * per)], axis=0
        )
        outs.append(dot(inner.astype(bf16), down_ref[e]).astype(bf16))
    out_ref[...] = dot(back_ref[...], jnp.concatenate(outs, axis=0)).astype(bf16)
    normed = rounded(centred_ref[...] * inv_ref[...] * gain_ref[...])
    lane = iota((rows, lanes), 1)
    tiles = []
    for t in range(hidden // lanes):
        tile = jnp.zeros((rows, lanes), f32)
        for k in range(lanes // share):
            piece = inner_ref[t * (lanes // share) + k, :, hidden:].astype(f32)
            tile = jnp.where(lane // share == k, pltpu.roll(piece, k * share, 1), tile)
        tiles.append(tile)
    shared = jnp.concatenate(tiles, axis=1).astype(bf16)
    base_ref[...] = res_scale * normed + dot(shared, shared_ref[...])


def combine(got_ref, high_ref, low_ref, base_ref, resid_ref, stats_ref):
    got = got_ref[...]
    resid = base_ref[...] + dot(high_ref[...], got) + dot(low_ref[...], got)
    resid_ref[...] = resid
    column = jnp.sum(resid, axis=1, keepdims=True)
    squares = jnp.sum(resid * resid, axis=1, keepdims=True)
    at, lane = iota(resid.shape, 0), iota(resid.shape, 1)
    half = lanes // 2
    seen = jnp.where(lane == at, column, jnp.where(lane == at + half, squares, 0.0))
    row = jnp.sum(seen, axis=0, keepdims=True)
    for j in range(stats_ref.shape[0]):
        stats_ref[j] = row


def finish(got_ref, resid_ref, gain_ref, out_ref, width):
    total = jnp.sum(got_ref[...], axis=0)
    at, lane = iota(resid_ref.shape, 0), iota(resid_ref.shape, 1)

    def column(start):
        return jnp.sum(jnp.where(lane == at + start, total, 0.0), axis=1, keepdims=True)

    mean = column(0) / width
    spread = column(lanes // 2) / width - mean * mean
    out_ref[...] = (
        (resid_ref[...] - mean) * lax.rsqrt(spread + norm_eps) * gain_ref[...]
    ).astype(bf16)


def to_each(value, axis):
    return lax.all_to_all(value, axis, split_axis=0, concat_axis=0, tiled=True)


def per_device(
    tokens,
    state,
    w_query,
    w_key,
    w_value,
    w_outgate,
    decay_down,
    decay_up,
    decay_bias,
    head_gain,
    w_output,
    norm1_gain,
    route_ids,
    route_weight,
    exp_gate,
    exp_up,
    exp_down,
    sh_gate,
    sh_up,
    sh_down,
    norm2_gain,
):
    rows, width = tokens.shape
    tp_count, ep_count = lax.axis_size("tp"), lax.axis_size("ep")
    cols = width // tp_count
    hidden = exp_gate.shape[2]
    per_block = exp_gate.shape[0] * capacity
    slots = ep_count * per_block
    gain1, gain2 = norm1_gain.reshape(1, cols), norm2_gain.reshape(1, cols)

    held = (
        route_ids.T,
        route_weight.T,
        tokens,
        decay_down.T,
        decay_up,
        decay_bias.reshape(1, -1),
        w_query,
        w_key,
        w_value,
        w_outgate,
        head_gain.reshape(1, -1),
        state,
        w_output,
    )
    outgoing, send, high, low, perm, back, own = local_call(
        attend,
        (
            struct((tp_count, rows + 8, cols), bf16),
            struct((slots, lanes), bf16),
            struct((rows, slots), bf16),
            struct((rows, slots), bf16),
            struct((slots, slots), bf16),
            struct((slots, slots), bf16),
            struct((rows, cols), f32),
        ),
        held,
        stay=tuple(range(len(held))),
        scratch=[pltpu.VMEM(a.shape, a.dtype) for a in held]
        + [pltpu.SemaphoreType.DMA((len(held),))],
    )
    arrived = to_each(outgoing, "tp")

    def named(body):
        def call(*refs):
            body(*refs, width)

        call.__name__ = body.__name__
        return call

    sent, centred = local_call(
        named(dispatch),
        (struct((slots, cols), bf16), struct((rows, cols), f32)),
        (arrived, own, gain1, send),
    )
    taken = to_each(sent.reshape(ep_count, per_block, cols), "ep").reshape(slots, cols)
    block = struct((tp_count // 2, rows, 2 * hidden + lanes), bf16)
    keep, give = local_call(
        expand,
        (block, block),
        (taken, perm, exp_gate, exp_up, sh_gate, sh_up, gain1, centred),
    )
    other = lax.ppermute(give, "tp", [(i, i ^ 1) for i in range(tp_count)])
    partials = local_call(pair, block, (keep, other))
    same_core = [list(range(core, tp_count, 2)) for core in range(2)]
    parts = lax.all_to_all(partials, "tp", 0, 0, tiled=True, axis_index_groups=same_core)
    inner, inv = local_call(
        named(activate),
        (struct((rows, hidden + lanes), bf16), struct((rows, cols), f32)),
        (parts,),
    )
    inners = lax.all_gather(inner, "tp", axis=0)
    result, base = local_call(
        contract,
        (struct((slots, cols), bf16), struct((rows, cols), f32)),
        (inners, back, exp_down, sh_down, centred, gain1, inv),
    )
    returned = to_each(result.reshape(ep_count, per_block, cols), "ep").reshape(slots, cols)
    resid, stats = local_call(
        combine,
        (struct((rows, cols), f32), struct((tp_count, 1, lanes), f32)),
        (returned, high, low, base),
    )
    all_stats = to_each(stats, "tp")

    return local_call(
        named(finish), jax.ShapeDtypeStruct((rows, cols), bf16), (all_stats, resid, gain2)
    )


def solution(mesh):
    in_specs = (
        P("ep", None),
        P("ep", "tp", None, None),
        P(None, "tp"),
        P(None, "tp"),
        P(None, "tp"),
        P(None, "tp"),
        P(),
        P(None, "tp"),
        P("tp"),
        P(),
        P("tp", None),
        P("tp"),
        P("ep", None),
        P("ep", None),
        P("ep", "tp", None),
        P("ep", "tp", None),
        P("ep", None, "tp"),
        P("tp", None),
        P("tp", None),
        P(None, "tp"),
        P("tp"),
    )
    out_specs = P("ep", "tp")
    return jax.shard_map(
        per_device, mesh=mesh, in_specs=in_specs, out_specs=out_specs, check_vma=False
    )
```

```python
import jax
import jax.numpy as jnp
from jax import lax
from jax.experimental import pallas as pl
from jax.experimental.pallas import tpu as pltpu
from jax.sharding import PartitionSpec as P

res_scale = 2.0**0.5
decay_tau = 16.0
norm_eps = 1e-05
capacity = 2
lanes = 128

f32 = jnp.float32
bf16 = jnp.bfloat16


def local_call(body, outs, args, stay=(), scratch=()):
    vmem = pl.BlockSpec(memory_space=pltpu.VMEM)
    hbm = pl.BlockSpec(memory_space=pl.ANY)
    placed = [
        pltpu.with_memory_space_constraint(a, pltpu.HBM if k in stay else pltpu.VMEM)
        for k, a in enumerate(args)
    ]
    return pl.pallas_call(
        body,
        out_shape=outs,
        in_specs=[hbm if k in stay else vmem for k in range(len(args))],
        out_specs=jax.tree.map(lambda _: vmem, outs),
        scratch_shapes=scratch,
        compiler_params=pltpu.CompilerParams(vmem_limit_bytes=24 * 2**20),
        name=body.__name__,
    )(*placed)


def struct(shape, dtype):
    return pltpu.VMEM(shape, dtype)


def iota(shape, dim):
    return lax.broadcasted_iota(jnp.int32, shape, dim)


def dot(left, right):
    return jnp.dot(left, right, preferred_element_type=f32)


def rounded(value):
    return value.astype(bf16).astype(f32)


def as_row(column):
    rows = column.shape[0]
    seen = jnp.where(iota((rows, lanes), 0) == iota((rows, lanes), 1), column, 0.0)
    return jnp.sum(seen, axis=0, keepdims=True)


def as_column(row, rows):
    seen = jnp.where(iota((rows, lanes), 0) == iota((rows, lanes), 1), row, 0.0)
    return jnp.sum(seen, axis=1, keepdims=True)


def silu(value):
    return value * jax.nn.sigmoid(value)


def route(ids_ref, weight_ref, send_ref, high_ref, low_ref, perm_ref, back_ref):
    top, rows = ids_ref.shape
    slots = send_ref.shape[0]
    blocks = slots // (4 * capacity)

    def square(ref):
        wide = jnp.concatenate([ref[...].astype(f32), jnp.zeros((top, lanes - rows), f32)], axis=1)
        return jnp.concatenate([wide, jnp.zeros((lanes - top, lanes), f32)], axis=0)

    ids, weights = square(ids_ref), square(weight_ref)
    slot = iota((slots, lanes), 0)
    expert = jnp.where(iota((slots, lanes), 1) < rows, slot // capacity, -1).astype(f32)
    hit = jnp.zeros((slots, lanes), f32)
    for k in range(top):
        hit = jnp.where(ids[k : k + 1, :] == expert, 1.0, hit)
    earlier = (iota((lanes, lanes), 0) < iota((lanes, lanes), 1)).astype(bf16)
    rank = dot(hit.astype(bf16), earlier)
    send_ref[...] = jnp.where(rank == (slot % capacity).astype(f32), hit, 0.0).astype(bf16)
    ids, weights = ids.T, weights.T
    slot = iota((rows, slots), 1)
    expert = (slot // capacity).astype(f32)
    hit = jnp.zeros((rows, slots), f32)
    weight = jnp.zeros((rows, slots), f32)
    for k in range(top):
        same = ids[:rows, k : k + 1] == expert
        hit = jnp.where(same, 1.0, hit)
        weight = jnp.where(same, weights[:rows, k : k + 1], weight)
    earlier = (iota((rows, rows), 1) < iota((rows, rows), 0)).astype(bf16)
    rank = dot(earlier, hit.astype(bf16))
    weight = jnp.where(rank == (slot % capacity).astype(f32), weight, 0.0)
    high = weight.astype(bf16)
    high_ref[...] = high
    low_ref[...] = (weight - high.astype(f32)).astype(bf16)
    per_expert = blocks * capacity

    def source(at):
        expert, rest = at // per_expert, at % per_expert
        return rest // capacity * (4 * capacity) + expert * capacity + rest % capacity

    one, two = iota((slots, slots), 0), iota((slots, slots), 1)
    perm_ref[...] = (source(iota((slots, 1), 0)) == two).astype(bf16)
    back_ref[...] = (one == source(iota((1, slots), 1))).astype(bf16)


def attend(*refs):
    count, extra = 13, 4
    far, refs = refs[: count + extra], refs[count + extra :]
    out_ref, tables, own_ref, refs = refs[0], refs[1:6], refs[6], refs[7:]
    near, sems = refs[extra:-1] + refs[:extra], refs[-1]
    ids, weights, tok, dd, du, db, wq, wk, wv, wg, hg, state, wo = range(count)
    copies = [pltpu.make_async_copy(a, b, sems.at[k]) for k, (a, b) in enumerate(zip(far, near))]
    for copy in copies:
        copy.start()

    def ready(*which):
        for k in which:
            copies[k].wait()

    ready(ids, weights)
    route(near[ids], near[weights], *tables)
    ready(tok, dd, du, db)
    tok_ref = near[tok]
    rows, width = tok_ref.shape
    tokens = tok_ref[...]
    start = pl.multiple_of(lax.axis_index("tp") * lanes, lanes)
    mean = jnp.sum(tokens.astype(f32), axis=1, keepdims=True) / width
    own_ref[...] = res_scale * (tok_ref[:, pl.ds(start, lanes)].astype(f32) - mean)
    low = lax.dot_general(
        tokens, near[dd][...], (((1,), (1,)), ((), ())), preferred_element_type=f32
    ).astype(bf16)
    pre = dot(low, near[du][...]) + near[db][...]
    log_decay = (jnp.minimum(pre, 0.0) - jnp.log1p(jnp.exp(-jnp.abs(pre)))) / decay_tau
    decay = jnp.exp(log_decay)
    ready(wq)
    key_dim = near[wq].shape[1]
    queries = rounded(dot(tokens, near[wq][...])) * key_dim ** (-0.5)
    decayed = queries * decay
    turned = jnp.concatenate([decayed, jnp.zeros((lanes - rows, key_dim), f32)], axis=0).T
    ready(wk, wv)
    keys = rounded(dot(tokens, near[wk][...]))
    values = rounded(dot(tokens, near[wv][...]))
    ready(wg, hg, state)
    gate = rounded(dot(tokens, near[wg][...]))
    carried = jnp.concatenate(
        [
            jnp.sum(turned[:, b : b + 1] * near[state][b, 0], axis=0, keepdims=True)
            for b in range(rows)
        ],
        axis=0,
    )
    attended = carried + jnp.sum(queries * keys, axis=1, keepdims=True) * values
    inv_norm = lax.rsqrt(jnp.mean(attended * attended, axis=1, keepdims=True) + norm_eps)
    head_out = (attended * inv_norm * near[hg][...] * silu(gate)).astype(bf16)
    ready(wo)
    partial = rounded(dot(head_out, near[wo][...]))
    row = as_row(jnp.sum(partial, axis=1, keepdims=True))
    high = rounded(row)
    middle = rounded(row - high)
    low = row - high - middle
    at = iota((8, lanes), 0)
    tail = jnp.where(at == 0, high, jnp.where(at == 1, middle, jnp.where(at == 2, low, 0.0)))
    for j in range(out_ref.shape[0]):
        out_ref[j] = jnp.concatenate(
            [partial[:, j * lanes : (j + 1) * lanes], tail], axis=0
        ).astype(bf16)
    ready(*range(count, count + extra))


def dispatch(got_ref, own_ref, gain_ref, send_ref, rows_ref, centred_ref, width):
    rows = own_ref.shape[0]
    total = jnp.sum(got_ref[...].astype(f32), axis=0)
    mixed = rounded(total[:rows])
    sums = total[rows : rows + 1] + total[rows + 1 : rows + 2] + total[rows + 2 : rows + 3]
    centred = own_ref[...] + mixed - as_column(sums, rows) / width
    centred_ref[...] = centred
    scaled = centred * gain_ref[...]
    filled = jnp.concatenate([scaled, jnp.zeros((lanes - rows, lanes), f32)], axis=0)
    rows_ref[...] = dot(send_ref[...], filled.astype(bf16)).astype(bf16)


def two_parts(column):
    high = rounded(column)
    return high, column - high


def expand(
    rows_ref, perm_ref, gate_ref, up_ref, sg_ref, su_ref, gain_ref, centred_ref, keep_ref, send_ref
):
    pairs, rows, _ = keep_ref.shape
    experts, _, hidden = gate_ref.shape
    chunks = 2 * pairs
    even = lax.rem(lax.axis_index("tp"), 2) == 0
    sorted_rows = dot(perm_ref[...], rows_ref[...])
    scale = sorted_rows / gain_ref[...]
    high, low = two_parts(jnp.sum(scale * scale, axis=1, keepdims=True))
    centred = centred_ref[...]
    own_high, own_low = two_parts(jnp.sum(centred * centred, axis=1, keepdims=True))
    own = (centred * gain_ref[...]).astype(bf16)
    shared_gate, shared_up = dot(own, sg_ref[...]), dot(own, su_ref[...])
    lane = iota((rows, lanes), 1)
    share = hidden // chunks
    per = chunks // experts

    def last_block(j):
        tile = j * share // lanes * lanes
        turn = j * share % lanes
        g = pltpu.roll(shared_gate[:, tile : tile + lanes], (lanes - turn) % lanes, 1)
        u = pltpu.roll(shared_up[:, tile : tile + lanes], (lanes + share - turn) % lanes, 1)
        whole = slice(j * rows, (j + 1) * rows)
        last = jnp.where(lane < share, g, jnp.where(lane < 2 * share, u, 0.0))
        last = jnp.where(lane == 2 * share, high[whole], last)
        last = jnp.where(lane == 2 * share + 1, low[whole], last)
        last = jnp.where(lane == 2 * share + 2, own_high, last)
        return jnp.where(lane == 2 * share + 3, own_low, last)

    for e in range(experts):
        taken = sorted_rows[e * per * rows : (e + 1) * per * rows].astype(bf16)
        gate, up = dot(taken, gate_ref[e]), dot(taken, up_ref[e])
        for q in range(0, per, 2):
            j = e * per + q
            one, two = slice(q * rows, (q + 1) * rows), slice((q + 1) * rows, (q + 2) * rows)
            for at, a, b in (
                (slice(0, hidden), gate[one], gate[two]),
                (slice(hidden, 2 * hidden), up[one], up[two]),
                (slice(2 * hidden, 2 * hidden + lanes), last_block(j), last_block(j + 1)),
            ):
                keep_ref[j // 2, :, at] = jnp.where(even, a, b).astype(bf16)
                send_ref[j // 2, :, at] = jnp.where(even, b, a).astype(bf16)


def pair(keep_ref, got_ref, out_ref):
    pairs, rows, width = keep_ref.shape
    wide = width - lanes
    out_ref[:, :, :wide] = keep_ref[:, :, :wide] + got_ref[:, :, :wide]
    last = keep_ref[:, :, wide:].astype(f32) + got_ref[:, :, wide:].astype(f32)
    lane = iota(last.shape, 2)
    share = wide // 2 // (2 * pairs)
    for at in (2 * share, 2 * share + 2):
        high, low = two_parts(last[:, :, at : at + 1] + last[:, :, at + 1 : at + 2])
        last = jnp.where(lane == at, high, jnp.where(lane == at + 1, low, last))
    out_ref[:, :, wide:] = last.astype(bf16)


def activate(got_ref, inner_ref, own_ref, width):
    rows = got_ref.shape[1]
    chunks = 2 * got_ref.shape[0]
    hidden = inner_ref.shape[1] - lanes
    share = hidden // chunks
    total = jnp.sum(got_ref[...].astype(f32), axis=0)
    last = total[:, 2 * hidden :]

    def inv_std(at):
        squares = last[:, at : at + 1] + last[:, at + 1 : at + 2]
        return lax.rsqrt(squares / width + norm_eps)

    inv = inv_std(2 * share)
    gate = rounded(total[:, :hidden] * inv)
    up = rounded(total[:, hidden : 2 * hidden] * inv)
    inner_ref[:, :hidden] = (silu(gate) * up).astype(bf16)
    inv = inv_std(2 * share + 2)
    own_ref[...] = jnp.broadcast_to(inv, own_ref.shape)
    both = rounded(last * inv)
    up = pltpu.roll(both, lanes - share, 1)
    lane = iota((rows, lanes), 1)
    inner_ref[:, hidden:] = jnp.where(lane < share, silu(both) * up, 0.0).astype(bf16)


def contract(inner_ref, back_ref, down_ref, shared_ref, centred_ref, gain_ref, inv_ref, out_ref, base_ref):
    experts, hidden, _ = down_ref.shape
    chunks, rows, _ = inner_ref.shape
    per = chunks // experts
    share = hidden // chunks
    outs = []
    for e in range(experts):
        inner = jnp.concatenate(
            [inner_ref[j, :, :hidden].astype(f32) for j in range(e * per, (e + 1) * per)], axis=0
        )
        outs.append(dot(inner.astype(bf16), down_ref[e]).astype(bf16))
    out_ref[...] = dot(back_ref[...], jnp.concatenate(outs, axis=0)).astype(bf16)
    normed = rounded(centred_ref[...] * inv_ref[...] * gain_ref[...])
    lane = iota((rows, lanes), 1)
    tiles = []
    for t in range(hidden // lanes):
        tile = jnp.zeros((rows, lanes), f32)
        for k in range(lanes // share):
            piece = inner_ref[t * (lanes // share) + k, :, hidden:].astype(f32)
            tile = jnp.where(lane // share == k, pltpu.roll(piece, k * share, 1), tile)
        tiles.append(tile)
    shared = jnp.concatenate(tiles, axis=1).astype(bf16)
    base_ref[...] = res_scale * normed + dot(shared, shared_ref[...])


def combine(got_ref, high_ref, low_ref, base_ref, resid_ref, stats_ref):
    got = got_ref[...]
    resid = base_ref[...] + dot(high_ref[...], got) + dot(low_ref[...], got)
    resid_ref[...] = resid
    column = jnp.sum(resid, axis=1, keepdims=True)
    squares = jnp.sum(resid * resid, axis=1, keepdims=True)
    at, lane = iota(resid.shape, 0), iota(resid.shape, 1)
    half = lanes // 2
    seen = jnp.where(lane == at, column, jnp.where(lane == at + half, squares, 0.0))
    row = jnp.sum(seen, axis=0, keepdims=True)
    for j in range(stats_ref.shape[0]):
        stats_ref[j] = row


def finish(got_ref, resid_ref, gain_ref, out_ref, width):
    total = jnp.sum(got_ref[...], axis=0)
    at, lane = iota(resid_ref.shape, 0), iota(resid_ref.shape, 1)

    def column(start):
        return jnp.sum(jnp.where(lane == at + start, total, 0.0), axis=1, keepdims=True)

    mean = column(0) / width
    spread = column(lanes // 2) / width - mean * mean
    out_ref[...] = (
        (resid_ref[...] - mean) * lax.rsqrt(spread + norm_eps) * gain_ref[...]
    ).astype(bf16)


def to_each(value, axis):
    return lax.all_to_all(value, axis, split_axis=0, concat_axis=0, tiled=True)


def per_device(
    tokens,
    state,
    w_query,
    w_key,
    w_value,
    w_outgate,
    decay_down,
    decay_up,
    decay_bias,
    head_gain,
    w_output,
    norm1_gain,
    route_ids,
    route_weight,
    exp_gate,
    exp_up,
    exp_down,
    sh_gate,
    sh_up,
    sh_down,
    norm2_gain,
):
    rows, width = tokens.shape
    tp_count, ep_count = lax.axis_size("tp"), lax.axis_size("ep")
    cols = width // tp_count
    hidden = exp_gate.shape[2]
    per_block = exp_gate.shape[0] * capacity
    slots = ep_count * per_block
    gain1, gain2 = norm1_gain.reshape(1, cols), norm2_gain.reshape(1, cols)

    held = (
        route_ids.T,
        route_weight.T,
        tokens,
        decay_down.T,
        decay_up,
        decay_bias.reshape(1, -1),
        w_query,
        w_key,
        w_value,
        w_outgate,
        head_gain.reshape(1, -1),
        state,
        w_output,
    )
    later = (exp_gate, exp_up, sh_gate, sh_up)
    outgoing, send, high, low, perm, back, own, *later = local_call(
        attend,
        (
            struct((tp_count, rows + 8, cols), bf16),
            struct((slots, lanes), bf16),
            struct((rows, slots), bf16),
            struct((rows, slots), bf16),
            struct((slots, slots), bf16),
            struct((slots, slots), bf16),
            struct((rows, cols), f32),
            *(struct(a.shape, a.dtype) for a in later),
        ),
        held + later,
        stay=tuple(range(len(held + later))),
        scratch=[pltpu.VMEM(a.shape, a.dtype) for a in held]
        + [pltpu.SemaphoreType.DMA((len(held + later),))],
    )
    arrived = to_each(outgoing, "tp")

    def named(body):
        def call(*refs):
            body(*refs, width)

        call.__name__ = body.__name__
        return call

    sent, centred = local_call(
        named(dispatch),
        (struct((slots, cols), bf16), struct((rows, cols), f32)),
        (arrived, own, gain1, send),
    )
    taken = to_each(sent.reshape(ep_count, per_block, cols), "ep").reshape(slots, cols)
    block = struct((tp_count // 2, rows, 2 * hidden + lanes), bf16)
    keep, give = local_call(
        expand,
        (block, block),
        (taken, perm, *later, gain1, centred),
    )
    other = lax.ppermute(give, "tp", [(i, i ^ 1) for i in range(tp_count)])
    partials = local_call(pair, block, (keep, other))
    same_core = [list(range(core, tp_count, 2)) for core in range(2)]
    parts = lax.all_to_all(partials, "tp", 0, 0, tiled=True, axis_index_groups=same_core)
    inner, inv = local_call(
        named(activate),
        (struct((rows, hidden + lanes), bf16), struct((rows, cols), f32)),
        (parts,),
    )
    inners = lax.all_gather(inner, "tp", axis=0)
    result, base = local_call(
        contract,
        (struct((slots, cols), bf16), struct((rows, cols), f32)),
        (inners, back, exp_down, sh_down, centred, gain1, inv),
    )
    returned = to_each(result.reshape(ep_count, per_block, cols), "ep").reshape(slots, cols)
    resid, stats = local_call(
        combine,
        (struct((rows, cols), f32), struct((tp_count, 1, lanes), f32)),
        (returned, high, low, base),
    )
    all_stats = to_each(stats, "tp")

    return local_call(
        named(finish), jax.ShapeDtypeStruct((rows, cols), bf16), (all_stats, resid, gain2)
    )


def solution(mesh):
    in_specs = (
        P("ep", None),
        P("ep", "tp", None, None),
        P(None, "tp"),
        P(None, "tp"),
        P(None, "tp"),
        P(None, "tp"),
        P(),
        P(None, "tp"),
        P("tp"),
        P(),
        P("tp", None),
        P("tp"),
        P("ep", None),
        P("ep", None),
        P("ep", "tp", None),
        P("ep", "tp", None),
        P("ep", None, "tp"),
        P("tp", None),
        P("tp", None),
        P(None, "tp"),
        P("tp"),
    )
    out_specs = P("ep", "tp")
    return jax.shard_map(
        per_device, mesh=mesh, in_specs=in_specs, out_specs=out_specs, check_vma=False
    )
```

```python
import jax
import jax.numpy as jnp
from jax import lax
from jax.experimental import pallas as pl
from jax.experimental.pallas import tpu as pltpu
from jax.sharding import PartitionSpec as P

res_scale = 2.0**0.5
decay_tau = 16.0
norm_eps = 1e-05
capacity = 2
lanes = 128

f32 = jnp.float32
bf16 = jnp.bfloat16


def local_call(body, outs, args, stay=(), scratch=()):
    vmem = pl.BlockSpec(memory_space=pltpu.VMEM)
    hbm = pl.BlockSpec(memory_space=pl.ANY)
    placed = [
        pltpu.with_memory_space_constraint(a, pltpu.HBM if k in stay else pltpu.VMEM)
        for k, a in enumerate(args)
    ]
    return pl.pallas_call(
        body,
        out_shape=outs,
        in_specs=[hbm if k in stay else vmem for k in range(len(args))],
        out_specs=jax.tree.map(lambda _: vmem, outs),
        scratch_shapes=scratch,
        compiler_params=pltpu.CompilerParams(vmem_limit_bytes=24 * 2**20),
        name=body.__name__,
    )(*placed)


def struct(shape, dtype):
    return pltpu.VMEM(shape, dtype)


def iota(shape, dim):
    return lax.broadcasted_iota(jnp.int32, shape, dim)


def dot(left, right):
    return jnp.dot(left, right, preferred_element_type=f32)


def rounded(value):
    return value.astype(bf16).astype(f32)


def as_row(column):
    rows = column.shape[0]
    seen = jnp.where(iota((rows, lanes), 0) == iota((rows, lanes), 1), column, 0.0)
    return jnp.sum(seen, axis=0, keepdims=True)


def as_column(row, rows):
    seen = jnp.where(iota((rows, lanes), 0) == iota((rows, lanes), 1), row, 0.0)
    return jnp.sum(seen, axis=1, keepdims=True)


def silu(value):
    return value * jax.nn.sigmoid(value)


def route(ids_ref, weight_ref, send_ref, high_ref, low_ref, perm_ref, back_ref):
    top, rows = ids_ref.shape
    slots = send_ref.shape[0]
    blocks = slots // (4 * capacity)

    def square(ref):
        wide = jnp.concatenate([ref[...].astype(f32), jnp.zeros((top, lanes - rows), f32)], axis=1)
        return jnp.concatenate([wide, jnp.zeros((lanes - top, lanes), f32)], axis=0)

    ids, weights = square(ids_ref), square(weight_ref)
    slot = iota((slots, lanes), 0)
    expert = jnp.where(iota((slots, lanes), 1) < rows, slot // capacity, -1).astype(f32)
    hit = jnp.zeros((slots, lanes), f32)
    for k in range(top):
        hit = jnp.where(ids[k : k + 1, :] == expert, 1.0, hit)
    earlier = (iota((lanes, lanes), 0) < iota((lanes, lanes), 1)).astype(bf16)
    rank = dot(hit.astype(bf16), earlier)
    send_ref[...] = jnp.where(rank == (slot % capacity).astype(f32), hit, 0.0).astype(bf16)
    ids, weights = ids.T, weights.T
    slot = iota((rows, slots), 1)
    expert = (slot // capacity).astype(f32)
    hit = jnp.zeros((rows, slots), f32)
    weight = jnp.zeros((rows, slots), f32)
    for k in range(top):
        same = ids[:rows, k : k + 1] == expert
        hit = jnp.where(same, 1.0, hit)
        weight = jnp.where(same, weights[:rows, k : k + 1], weight)
    earlier = (iota((rows, rows), 1) < iota((rows, rows), 0)).astype(bf16)
    rank = dot(earlier, hit.astype(bf16))
    weight = jnp.where(rank == (slot % capacity).astype(f32), weight, 0.0)
    high = weight.astype(bf16)
    high_ref[...] = high
    low_ref[...] = (weight - high.astype(f32)).astype(bf16)
    per_expert = blocks * capacity

    def source(at):
        expert, rest = at // per_expert, at % per_expert
        return rest // capacity * (4 * capacity) + expert * capacity + rest % capacity

    one, two = iota((slots, slots), 0), iota((slots, slots), 1)
    perm_ref[...] = (source(iota((slots, 1), 0)) == two).astype(bf16)
    back_ref[...] = (one == source(iota((1, slots), 1))).astype(bf16)


def attend(*refs):
    count, extra = 13, 4
    far, refs = refs[: count + extra], refs[count + extra :]
    out_ref, tables, own_ref, refs = refs[0], refs[1:6], refs[6], refs[7:]
    near, sems = refs[extra:-1] + refs[:extra], refs[-1]
    ids, weights, tok, dd, du, db, wq, wk, wv, wg, hg, state, wo = range(count)
    copies = [pltpu.make_async_copy(a, b, sems.at[k]) for k, (a, b) in enumerate(zip(far, near))]
    for copy in copies:
        copy.start()

    def ready(*which):
        for k in which:
            copies[k].wait()

    ready(ids, weights)
    route(near[ids], near[weights], *tables)
    ready(tok, dd, du, db)
    tok_ref = near[tok]
    rows, width = tok_ref.shape
    tokens = tok_ref[...]
    start = pl.multiple_of(lax.axis_index("tp") * lanes, lanes)
    mean = jnp.sum(tokens.astype(f32), axis=1, keepdims=True) / width
    own_ref[...] = res_scale * (tok_ref[:, pl.ds(start, lanes)].astype(f32) - mean)
    low = lax.dot_general(
        tokens, near[dd][...], (((1,), (1,)), ((), ())), preferred_element_type=f32
    ).astype(bf16)
    pre = dot(low, near[du][...]) + near[db][...]
    log_decay = (jnp.minimum(pre, 0.0) - jnp.log1p(jnp.exp(-jnp.abs(pre)))) / decay_tau
    decay = jnp.exp(log_decay)
    ready(wq)
    key_dim = near[wq].shape[1]
    queries = rounded(dot(tokens, near[wq][...])) * key_dim ** (-0.5)
    decayed = queries * decay
    turned = jnp.concatenate([decayed, jnp.zeros((lanes - rows, key_dim), f32)], axis=0).T
    ready(wk, wv)
    keys = rounded(dot(tokens, near[wk][...]))
    values = rounded(dot(tokens, near[wv][...]))
    ready(wg, hg, state)
    gate = rounded(dot(tokens, near[wg][...]))
    carried = jnp.concatenate(
        [
            jnp.sum(turned[:, b : b + 1] * near[state][b, 0], axis=0, keepdims=True)
            for b in range(rows)
        ],
        axis=0,
    )
    attended = carried + jnp.sum(queries * keys, axis=1, keepdims=True) * values
    inv_norm = lax.rsqrt(jnp.mean(attended * attended, axis=1, keepdims=True) + norm_eps)
    head_out = (attended * inv_norm * near[hg][...] * silu(gate)).astype(bf16)
    ready(wo)
    partial = rounded(dot(head_out, near[wo][...]))
    row = as_row(jnp.sum(partial, axis=1, keepdims=True))
    high = rounded(row)
    middle = rounded(row - high)
    low = row - high - middle
    at = iota((8, lanes), 0)
    tail = jnp.where(at == 0, high, jnp.where(at == 1, middle, jnp.where(at == 2, low, 0.0)))
    for j in range(out_ref.shape[0]):
        out_ref[j] = jnp.concatenate(
            [partial[:, j * lanes : (j + 1) * lanes], tail], axis=0
        ).astype(bf16)
    ready(*range(count, count + extra))


def dispatch(got_ref, own_ref, gain_ref, send_ref, rows_ref, centred_ref, width):
    rows = own_ref.shape[0]
    total = jnp.sum(got_ref[...].astype(f32), axis=0)
    mixed = rounded(total[:rows])
    sums = total[rows : rows + 1] + total[rows + 1 : rows + 2] + total[rows + 2 : rows + 3]
    centred = own_ref[...] + mixed - as_column(sums, rows) / width
    centred_ref[...] = centred
    scaled = centred * gain_ref[...]
    filled = jnp.concatenate([scaled, jnp.zeros((lanes - rows, lanes), f32)], axis=0)
    rows_ref[...] = dot(send_ref[...], filled.astype(bf16)).astype(bf16)


def two_parts(column):
    high = rounded(column)
    return high, column - high


def expand(
    rows_ref, perm_ref, gate_ref, up_ref, sg_ref, su_ref, gain_ref, centred_ref, keep_ref, send_ref
):
    pairs, _, _ = keep_ref.shape
    rows = centred_ref.shape[0]
    experts, _, hidden = gate_ref.shape
    chunks = 2 * pairs
    even = lax.rem(lax.axis_index("tp"), 2) == 0
    sorted_rows = dot(perm_ref[...], rows_ref[...])
    scale = sorted_rows / gain_ref[...]
    squares = jnp.sum(scale * scale, axis=1, keepdims=True)
    centred = centred_ref[...]
    own_sums = stat_rows(jnp.sum(centred * centred, axis=1, keepdims=True))
    own = (centred * gain_ref[...]).astype(bf16)
    shared_gate, shared_up = dot(own, sg_ref[...]), dot(own, su_ref[...])
    share = hidden // chunks
    per = chunks // experts
    tiles = hidden // lanes

    def last_block(j):
        tile = j * share // lanes * lanes
        turn = j * share % lanes
        g = pltpu.roll(shared_gate[:, tile : tile + lanes], (lanes - turn) % lanes, 1)
        u = pltpu.roll(shared_up[:, tile : tile + lanes], (lanes + share - turn) % lanes, 1)
        both = jnp.where(iota((rows, lanes), 1) < share, g, u)
        sums = stat_rows(squares[j * rows : (j + 1) * rows])
        return folded(both, sums, own_sums)

    for e in range(experts):
        taken = sorted_rows[e * per * rows : (e + 1) * per * rows].astype(bf16)
        gate, up = dot(taken, gate_ref[e]), dot(taken, up_ref[e])
        for q in range(0, per, 2):
            j = e * per + q
            one, two = slice(q * rows, (q + 1) * rows), slice((q + 1) * rows, (q + 2) * rows)
            for k in range(2 * tiles):
                part = gate if k < tiles else up
                at = slice(k % tiles * lanes, (k % tiles + 1) * lanes)
                here = slice(k * rows, (k + 1) * rows)
                a, b = part[one, at], part[two, at]
                keep_ref[j // 2, here] = jnp.where(even, a, b).astype(bf16)
                send_ref[j // 2, here] = jnp.where(even, b, a).astype(bf16)
            a, b = last_block(j), last_block(j + 1)
            here = slice(2 * tiles * rows, 2 * tiles * rows + 16)
            keep_ref[j // 2, here] = jnp.where(even, a, b).astype(bf16)
            send_ref[j // 2, here] = jnp.where(even, b, a).astype(bf16)


def stat_rows(column):
    shape = (column.shape[0], lanes)
    seen = jnp.where(iota(shape, 1) == iota(shape, 0) + lanes // 2, column, 0.0)
    return two_parts(jnp.sum(seen, axis=0, keepdims=True))


def folded(both, sums, own_sums):
    lane, at = iota((8, lanes), 1), iota((8, lanes), 0)
    upper = lane >= lanes // 2
    first = jnp.where(upper, pltpu.roll(both[16:24], lanes // 2, 1), both[0:8])
    stats = jnp.zeros((8, lanes), f32)
    for k, row in enumerate((*sums, *own_sums)):
        stats = jnp.where(at == k, row, stats)
    second = jnp.where(upper, stats, both[8:16])
    return jnp.concatenate([first, second], axis=0)


def pair(keep_ref, got_ref, out_ref):
    wide = keep_ref.shape[1] - 16
    out_ref[:, :wide] = keep_ref[:, :wide] + got_ref[:, :wide]
    for p in range(keep_ref.shape[0]):
        last = keep_ref[p, wide:].astype(f32) + got_ref[p, wide:].astype(f32)
        at, upper = iota(last.shape, 0), iota(last.shape, 1) >= lanes // 2
        for k in (8, 10):
            high, low = two_parts(last[k : k + 1] + last[k + 1 : k + 2])
            last = jnp.where(
                upper & (at == k), high, jnp.where(upper & (at == k + 1), low, last)
            )
        out_ref[p, wide:] = last.astype(bf16)


def activate(got_ref, inner_ref, own_ref, width):
    rows = own_ref.shape[0]
    chunks = 2 * got_ref.shape[0]
    tiles = (inner_ref.shape[0] - 8) // rows
    share = tiles * lanes // chunks
    total = jnp.sum(got_ref[...].astype(f32), axis=0)
    last = total[2 * tiles * rows :]

    def inv_std(at):
        shape = (rows, lanes)
        row = last[at : at + 1] + last[at + 1 : at + 2]
        seen = jnp.where(iota(shape, 1) == iota(shape, 0) + lanes // 2, row, 0.0)
        return lax.rsqrt(jnp.sum(seen, axis=1, keepdims=True) / width + norm_eps)

    inv = inv_std(8)
    for k in range(tiles):
        gate = rounded(total[k * rows : (k + 1) * rows] * inv)
        up = rounded(total[(tiles + k) * rows : (tiles + k + 1) * rows] * inv)
        inner_ref[k * rows : (k + 1) * rows] = (silu(gate) * up).astype(bf16)
    inv = inv_std(10)
    own_ref[...] = jnp.broadcast_to(inv, own_ref.shape)
    both = jnp.concatenate([last, pltpu.roll(last[0:8], lanes // 2, 1)], axis=0)
    both = rounded(both * inv)
    inner = silu(both) * pltpu.roll(both, lanes - share, 1)
    lane = iota((8, lanes), 1)
    packed = jnp.zeros((8, lanes), f32)
    for k in range(rows // 8):
        moved = pltpu.roll(inner[8 * k : 8 * k + 8], k * share, 1)
        packed = jnp.where(lane // share == k, moved, packed)
    inner_ref[tiles * rows :] = packed.astype(bf16)


def contract(inner_ref, back_ref, down_ref, shared_ref, centred_ref, gain_ref, inv_ref, out_ref, base_ref):
    experts, hidden, _ = down_ref.shape
    chunks = inner_ref.shape[0]
    rows = centred_ref.shape[0]
    per = chunks // experts
    width = hidden // lanes
    share = hidden // chunks
    outs = []
    for e in range(experts):
        inner = jnp.concatenate(
            [
                jnp.concatenate(
                    [inner_ref[j, k * rows : (k + 1) * rows].astype(f32) for k in range(width)],
                    axis=1,
                )
                for j in range(e * per, (e + 1) * per)
            ],
            axis=0,
        )
        outs.append(dot(inner.astype(bf16), down_ref[e]).astype(bf16))
    out_ref[...] = dot(back_ref[...], jnp.concatenate(outs, axis=0)).astype(bf16)
    normed = rounded(centred_ref[...] * inv_ref[...] * gain_ref[...])
    lane = iota((rows, lanes), 1)
    tiles = []
    for t in range(hidden // lanes):
        tile = jnp.zeros((rows, lanes), f32)
        for k in range(lanes // share):
            piece = inner_ref[t * (lanes // share) + k, width * rows :].astype(f32)
            turned = [
                pltpu.roll(piece, (k - b) * share % lanes, 1) for b in range(rows // 8)
            ]
            tile = jnp.where(lane // share == k, jnp.concatenate(turned, axis=0), tile)
        tiles.append(tile)
    shared = jnp.concatenate(tiles, axis=1).astype(bf16)
    base_ref[...] = res_scale * normed + dot(shared, shared_ref[...])


def combine(got_ref, high_ref, low_ref, base_ref, resid_ref, stats_ref):
    got = got_ref[...]
    resid = base_ref[...] + dot(high_ref[...], got) + dot(low_ref[...], got)
    resid_ref[...] = resid
    column = jnp.sum(resid, axis=1, keepdims=True)
    squares = jnp.sum(resid * resid, axis=1, keepdims=True)
    at, lane = iota(resid.shape, 0), iota(resid.shape, 1)
    half = lanes // 2
    seen = jnp.where(lane == at, column, jnp.where(lane == at + half, squares, 0.0))
    row = jnp.sum(seen, axis=0, keepdims=True)
    for j in range(stats_ref.shape[0]):
        stats_ref[j] = row


def finish(got_ref, resid_ref, gain_ref, out_ref, width):
    total = jnp.sum(got_ref[...], axis=0)
    at, lane = iota(resid_ref.shape, 0), iota(resid_ref.shape, 1)

    def column(start):
        return jnp.sum(jnp.where(lane == at + start, total, 0.0), axis=1, keepdims=True)

    mean = column(0) / width
    spread = column(lanes // 2) / width - mean * mean
    out_ref[...] = (
        (resid_ref[...] - mean) * lax.rsqrt(spread + norm_eps) * gain_ref[...]
    ).astype(bf16)


def to_each(value, axis):
    return lax.all_to_all(value, axis, split_axis=0, concat_axis=0, tiled=True)


def per_device(
    tokens,
    state,
    w_query,
    w_key,
    w_value,
    w_outgate,
    decay_down,
    decay_up,
    decay_bias,
    head_gain,
    w_output,
    norm1_gain,
    route_ids,
    route_weight,
    exp_gate,
    exp_up,
    exp_down,
    sh_gate,
    sh_up,
    sh_down,
    norm2_gain,
):
    rows, width = tokens.shape
    tp_count, ep_count = lax.axis_size("tp"), lax.axis_size("ep")
    cols = width // tp_count
    hidden = exp_gate.shape[2]
    per_block = exp_gate.shape[0] * capacity
    slots = ep_count * per_block
    gain1, gain2 = norm1_gain.reshape(1, cols), norm2_gain.reshape(1, cols)

    held = (
        route_ids.T,
        route_weight.T,
        tokens,
        decay_down.T,
        decay_up,
        decay_bias.reshape(1, -1),
        w_query,
        w_key,
        w_value,
        w_outgate,
        head_gain.reshape(1, -1),
        state,
        w_output,
    )
    later = (exp_gate, exp_up, sh_gate, sh_up)
    outgoing, send, high, low, perm, back, own, *later = local_call(
        attend,
        (
            struct((tp_count, rows + 8, cols), bf16),
            struct((slots, lanes), bf16),
            struct((rows, slots), bf16),
            struct((rows, slots), bf16),
            struct((slots, slots), bf16),
            struct((slots, slots), bf16),
            struct((rows, cols), f32),
            *(struct(a.shape, a.dtype) for a in later),
        ),
        held + later,
        stay=tuple(range(len(held + later))),
        scratch=[pltpu.VMEM(a.shape, a.dtype) for a in held]
        + [pltpu.SemaphoreType.DMA((len(held + later),))],
    )
    arrived = to_each(outgoing, "tp")

    def named(body):
        def call(*refs):
            body(*refs, width)

        call.__name__ = body.__name__
        return call

    sent, centred = local_call(
        named(dispatch),
        (struct((slots, cols), bf16), struct((rows, cols), f32)),
        (arrived, own, gain1, send),
    )
    taken = to_each(sent.reshape(ep_count, per_block, cols), "ep").reshape(slots, cols)
    tiles = hidden // lanes
    block = struct((tp_count // 2, 2 * tiles * rows + 16, lanes), bf16)
    keep, give = local_call(
        expand,
        (block, block),
        (taken, perm, *later, gain1, centred),
    )
    other = lax.ppermute(give, "tp", [(i, i ^ 1) for i in range(tp_count)])
    partials = local_call(pair, block, (keep, other))
    same_core = [list(range(core, tp_count, 2)) for core in range(2)]
    parts = lax.all_to_all(partials, "tp", 0, 0, tiled=True, axis_index_groups=same_core)
    inner, inv = local_call(
        named(activate),
        (struct((tiles * rows + 8, lanes), bf16), struct((rows, cols), f32)),
        (parts,),
    )
    inners = lax.all_gather(inner, "tp", axis=0)
    result, base = local_call(
        contract,
        (struct((slots, cols), bf16), struct((rows, cols), f32)),
        (inners, back, exp_down, sh_down, centred, gain1, inv),
    )
    returned = to_each(result.reshape(ep_count, per_block, cols), "ep").reshape(slots, cols)
    resid, stats = local_call(
        combine,
        (struct((rows, cols), f32), struct((tp_count, 1, lanes), f32)),
        (returned, high, low, base),
    )
    all_stats = to_each(stats, "tp")

    return local_call(
        named(finish), jax.ShapeDtypeStruct((rows, cols), bf16), (all_stats, resid, gain2)
    )


def solution(mesh):
    in_specs = (
        P("ep", None),
        P("ep", "tp", None, None),
        P(None, "tp"),
        P(None, "tp"),
        P(None, "tp"),
        P(None, "tp"),
        P(),
        P(None, "tp"),
        P("tp"),
        P(),
        P("tp", None),
        P("tp"),
        P("ep", None),
        P("ep", None),
        P("ep", "tp", None),
        P("ep", "tp", None),
        P("ep", None, "tp"),
        P("tp", None),
        P("tp", None),
        P(None, "tp"),
        P("tp"),
    )
    out_specs = P("ep", "tp")
    return jax.shard_map(
        per_device, mesh=mesh, in_specs=in_specs, out_specs=out_specs, check_vma=False
    )
```

```python
import jax
import jax.numpy as jnp
from jax import lax
from jax.experimental import pallas as pl
from jax.experimental.pallas import tpu as pltpu
from jax.sharding import PartitionSpec as P

res_scale = 2.0**0.5
decay_tau = 16.0
norm_eps = 1e-05
capacity = 2
lanes = 128

f32 = jnp.float32
bf16 = jnp.bfloat16


def local_call(body, outs, args, stay=(), scratch=()):
    vmem = pl.BlockSpec(memory_space=pltpu.VMEM)
    hbm = pl.BlockSpec(memory_space=pl.ANY)
    placed = [
        pltpu.with_memory_space_constraint(a, pltpu.HBM if k in stay else pltpu.VMEM)
        for k, a in enumerate(args)
    ]
    return pl.pallas_call(
        body,
        out_shape=outs,
        in_specs=[hbm if k in stay else vmem for k in range(len(args))],
        out_specs=jax.tree.map(lambda _: vmem, outs),
        scratch_shapes=scratch,
        compiler_params=pltpu.CompilerParams(vmem_limit_bytes=24 * 2**20),
        name=body.__name__,
    )(*placed)


def struct(shape, dtype):
    return pltpu.VMEM(shape, dtype)


def iota(shape, dim):
    return lax.broadcasted_iota(jnp.int32, shape, dim)


def dot(left, right):
    return jnp.dot(left, right, preferred_element_type=f32)


def rounded(value):
    return value.astype(bf16).astype(f32)


def as_row(column):
    rows = column.shape[0]
    seen = jnp.where(iota((rows, lanes), 0) == iota((rows, lanes), 1), column, 0.0)
    return jnp.sum(seen, axis=0, keepdims=True)


def as_column(row, rows):
    seen = jnp.where(iota((rows, lanes), 0) == iota((rows, lanes), 1), row, 0.0)
    return jnp.sum(seen, axis=1, keepdims=True)


def silu(value):
    return value * jax.nn.sigmoid(value)


def route(ids_ref, weight_ref, send_ref, high_ref, low_ref, perm_ref, back_ref):
    top, rows = ids_ref.shape
    slots = send_ref.shape[0]
    blocks = slots // (4 * capacity)

    def square(ref):
        wide = jnp.concatenate([ref[...].astype(f32), jnp.zeros((top, lanes - rows), f32)], axis=1)
        return jnp.concatenate([wide, jnp.zeros((lanes - top, lanes), f32)], axis=0)

    ids, weights = square(ids_ref), square(weight_ref)
    slot = iota((slots, lanes), 0)
    expert = jnp.where(iota((slots, lanes), 1) < rows, slot // capacity, -1).astype(f32)
    hit = jnp.zeros((slots, lanes), f32)
    for k in range(top):
        hit = jnp.where(ids[k : k + 1, :] == expert, 1.0, hit)
    earlier = (iota((lanes, lanes), 0) < iota((lanes, lanes), 1)).astype(bf16)
    rank = dot(hit.astype(bf16), earlier)
    send_ref[...] = jnp.where(rank == (slot % capacity).astype(f32), hit, 0.0).astype(bf16)
    ids, weights = ids.T, weights.T
    slot = iota((rows, slots), 1)
    expert = (slot // capacity).astype(f32)
    hit = jnp.zeros((rows, slots), f32)
    weight = jnp.zeros((rows, slots), f32)
    for k in range(top):
        same = ids[:rows, k : k + 1] == expert
        hit = jnp.where(same, 1.0, hit)
        weight = jnp.where(same, weights[:rows, k : k + 1], weight)
    earlier = (iota((rows, rows), 1) < iota((rows, rows), 0)).astype(bf16)
    rank = dot(earlier, hit.astype(bf16))
    weight = jnp.where(rank == (slot % capacity).astype(f32), weight, 0.0)
    high = weight.astype(bf16)
    high_ref[...] = high
    low_ref[...] = (weight - high.astype(f32)).astype(bf16)
    per_expert = blocks * capacity

    def source(at):
        expert, rest = at // per_expert, at % per_expert
        return rest // capacity * (4 * capacity) + expert * capacity + rest % capacity

    one, two = iota((slots, slots), 0), iota((slots, slots), 1)
    perm_ref[...] = (source(iota((slots, 1), 0)) == two).astype(bf16)
    back_ref[...] = (one == source(iota((1, slots), 1))).astype(bf16)


def attend(*refs):
    count, extra = 13, 4
    far, refs = refs[: count + extra], refs[count + extra :]
    out_ref, tables, own_ref, refs = refs[0], refs[1:6], refs[6], refs[7:]
    near, sems = refs[extra:-1] + refs[:extra], refs[-1]
    ids, weights, tok, dd, du, db, wq, wk, wv, wg, hg, state, wo = range(count)
    copies = {
        k: pltpu.make_async_copy(a, b, sems.at[k])
        for k, (a, b) in enumerate(zip(far, near))
        if k != wo
    }
    half = near[wo].shape[1] // 2
    halves = [
        pltpu.make_async_copy(far[wo].at[:, cut], near[wo].at[:, cut], sems.at[at])
        for cut, at in ((pl.ds(0, half), wo), (pl.ds(half, half), count + extra))
    ]
    for k in range(count + extra):
        for copy in halves if k == wo else (copies[k],):
            copy.start()

    def ready(*which):
        for k in which:
            copies[k].wait()

    ready(ids, weights)
    route(near[ids], near[weights], *tables)
    ready(tok, dd, du, db)
    tok_ref = near[tok]
    rows, width = tok_ref.shape
    tokens = tok_ref[...]
    start = pl.multiple_of(lax.axis_index("tp") * lanes, lanes)
    mean = jnp.sum(tokens.astype(f32), axis=1, keepdims=True) / width
    own_ref[...] = res_scale * (tok_ref[:, pl.ds(start, lanes)].astype(f32) - mean)
    low = lax.dot_general(
        tokens, near[dd][...], (((1,), (1,)), ((), ())), preferred_element_type=f32
    ).astype(bf16)
    pre = dot(low, near[du][...]) + near[db][...]
    log_decay = (jnp.minimum(pre, 0.0) - jnp.log1p(jnp.exp(-jnp.abs(pre)))) / decay_tau
    decay = jnp.exp(log_decay)
    ready(wq)
    key_dim = near[wq].shape[1]
    queries = rounded(dot(tokens, near[wq][...])) * key_dim ** (-0.5)
    decayed = queries * decay
    turned = jnp.concatenate([decayed, jnp.zeros((lanes - rows, key_dim), f32)], axis=0).T
    ready(wk, wv)
    keys = rounded(dot(tokens, near[wk][...]))
    values = rounded(dot(tokens, near[wv][...]))
    ready(wg, hg, state)
    gate = rounded(dot(tokens, near[wg][...]))
    carried = jnp.concatenate(
        [
            jnp.sum(turned[:, b : b + 1] * near[state][b, 0], axis=0, keepdims=True)
            for b in range(rows)
        ],
        axis=0,
    )
    attended = carried + jnp.sum(queries * keys, axis=1, keepdims=True) * values
    inv_norm = lax.rsqrt(jnp.mean(attended * attended, axis=1, keepdims=True) + norm_eps)
    head_out = (attended * inv_norm * near[hg][...] * silu(gate)).astype(bf16)
    partials = []
    for k, copy in enumerate(halves):
        copy.wait()
        partials.append(rounded(dot(head_out, near[wo][:, k * half : (k + 1) * half])))
    partial = jnp.concatenate(partials, axis=1)
    row = as_row(jnp.sum(partial, axis=1, keepdims=True))
    high = rounded(row)
    middle = rounded(row - high)
    low = row - high - middle
    at = iota((8, lanes), 0)
    tail = jnp.where(at == 0, high, jnp.where(at == 1, middle, jnp.where(at == 2, low, 0.0)))
    for j in range(out_ref.shape[0]):
        out_ref[j] = jnp.concatenate(
            [partial[:, j * lanes : (j + 1) * lanes], tail], axis=0
        ).astype(bf16)
    ready(*range(count, count + extra))


def dispatch(got_ref, own_ref, gain_ref, send_ref, rows_ref, centred_ref, width):
    rows = own_ref.shape[0]
    total = jnp.sum(got_ref[...].astype(f32), axis=0)
    mixed = rounded(total[:rows])
    sums = total[rows : rows + 1] + total[rows + 1 : rows + 2] + total[rows + 2 : rows + 3]
    centred = own_ref[...] + mixed - as_column(sums, rows) / width
    centred_ref[...] = centred
    scaled = centred * gain_ref[...]
    filled = jnp.concatenate([scaled, jnp.zeros((lanes - rows, lanes), f32)], axis=0)
    rows_ref[...] = dot(send_ref[...], filled.astype(bf16)).astype(bf16)


def two_parts(column):
    high = rounded(column)
    return high, column - high


def expand(
    rows_ref, perm_ref, gate_ref, up_ref, sg_ref, su_ref, gain_ref, centred_ref, keep_ref, send_ref
):
    pairs, _, _ = keep_ref.shape
    rows = centred_ref.shape[0]
    experts, _, hidden = gate_ref.shape
    chunks = 2 * pairs
    even = lax.rem(lax.axis_index("tp"), 2) == 0
    sorted_rows = dot(perm_ref[...], rows_ref[...])
    scale = sorted_rows / gain_ref[...]
    squares = jnp.sum(scale * scale, axis=1, keepdims=True)
    centred = centred_ref[...]
    own_sums = stat_rows(jnp.sum(centred * centred, axis=1, keepdims=True))
    own = (centred * gain_ref[...]).astype(bf16)
    shared_gate, shared_up = dot(own, sg_ref[...]), dot(own, su_ref[...])
    share = hidden // chunks
    per = chunks // experts
    tiles = hidden // lanes

    def last_block(j):
        tile = j * share // lanes * lanes
        turn = j * share % lanes
        g = pltpu.roll(shared_gate[:, tile : tile + lanes], (lanes - turn) % lanes, 1)
        u = pltpu.roll(shared_up[:, tile : tile + lanes], (lanes + share - turn) % lanes, 1)
        both = jnp.where(iota((rows, lanes), 1) < share, g, u)
        sums = stat_rows(squares[j * rows : (j + 1) * rows])
        return folded(both, sums, own_sums)

    for e in range(experts):
        taken = sorted_rows[e * per * rows : (e + 1) * per * rows].astype(bf16)
        gate, up = dot(taken, gate_ref[e]), dot(taken, up_ref[e])
        for q in range(0, per, 2):
            j = e * per + q
            one, two = slice(q * rows, (q + 1) * rows), slice((q + 1) * rows, (q + 2) * rows)
            for k in range(2 * tiles):
                part = gate if k < tiles else up
                at = slice(k % tiles * lanes, (k % tiles + 1) * lanes)
                here = slice(k * rows, (k + 1) * rows)
                a, b = part[one, at], part[two, at]
                keep_ref[j // 2, here] = jnp.where(even, a, b).astype(bf16)
                send_ref[j // 2, here] = jnp.where(even, b, a).astype(bf16)
            a, b = last_block(j), last_block(j + 1)
            here = slice(2 * tiles * rows, 2 * tiles * rows + 16)
            keep_ref[j // 2, here] = jnp.where(even, a, b).astype(bf16)
            send_ref[j // 2, here] = jnp.where(even, b, a).astype(bf16)


def stat_rows(column):
    shape = (column.shape[0], lanes)
    seen = jnp.where(iota(shape, 1) == iota(shape, 0) + lanes // 2, column, 0.0)
    return two_parts(jnp.sum(seen, axis=0, keepdims=True))


def folded(both, sums, own_sums):
    lane, at = iota((8, lanes), 1), iota((8, lanes), 0)
    upper = lane >= lanes // 2
    first = jnp.where(upper, pltpu.roll(both[16:24], lanes // 2, 1), both[0:8])
    stats = jnp.zeros((8, lanes), f32)
    for k, row in enumerate((*sums, *own_sums)):
        stats = jnp.where(at == k, row, stats)
    second = jnp.where(upper, stats, both[8:16])
    return jnp.concatenate([first, second], axis=0)


def pair(keep_ref, got_ref, out_ref):
    wide = keep_ref.shape[1] - 16
    out_ref[:, :wide] = keep_ref[:, :wide] + got_ref[:, :wide]
    for p in range(keep_ref.shape[0]):
        last = keep_ref[p, wide:].astype(f32) + got_ref[p, wide:].astype(f32)
        at, upper = iota(last.shape, 0), iota(last.shape, 1) >= lanes // 2
        for k in (8, 10):
            high, low = two_parts(last[k : k + 1] + last[k + 1 : k + 2])
            last = jnp.where(
                upper & (at == k), high, jnp.where(upper & (at == k + 1), low, last)
            )
        out_ref[p, wide:] = last.astype(bf16)


def activate(got_ref, inner_ref, own_ref, width):
    rows = own_ref.shape[0]
    chunks = 2 * got_ref.shape[0]
    tiles = (inner_ref.shape[0] - 8) // rows
    share = tiles * lanes // chunks
    total = jnp.sum(got_ref[...].astype(f32), axis=0)
    last = total[2 * tiles * rows :]

    def inv_std(at):
        shape = (rows, lanes)
        row = last[at : at + 1] + last[at + 1 : at + 2]
        seen = jnp.where(iota(shape, 1) == iota(shape, 0) + lanes // 2, row, 0.0)
        return lax.rsqrt(jnp.sum(seen, axis=1, keepdims=True) / width + norm_eps)

    inv = inv_std(8)
    for k in range(tiles):
        gate = rounded(total[k * rows : (k + 1) * rows] * inv)
        up = rounded(total[(tiles + k) * rows : (tiles + k + 1) * rows] * inv)
        inner_ref[k * rows : (k + 1) * rows] = (silu(gate) * up).astype(bf16)
    inv = inv_std(10)
    own_ref[...] = jnp.broadcast_to(inv, own_ref.shape)
    both = jnp.concatenate([last, pltpu.roll(last[0:8], lanes // 2, 1)], axis=0)
    both = rounded(both * inv)
    inner = silu(both) * pltpu.roll(both, lanes - share, 1)
    lane = iota((8, lanes), 1)
    packed = jnp.zeros((8, lanes), f32)
    for k in range(rows // 8):
        moved = pltpu.roll(inner[8 * k : 8 * k + 8], k * share, 1)
        packed = jnp.where(lane // share == k, moved, packed)
    inner_ref[tiles * rows :] = packed.astype(bf16)


def contract(inner_ref, back_ref, down_ref, shared_ref, centred_ref, gain_ref, inv_ref, out_ref, base_ref):
    experts, hidden, _ = down_ref.shape
    chunks = inner_ref.shape[0]
    rows = centred_ref.shape[0]
    per = chunks // experts
    width = hidden // lanes
    share = hidden // chunks
    outs = []
    for e in range(experts):
        inner = jnp.concatenate(
            [
                jnp.concatenate(
                    [inner_ref[j, k * rows : (k + 1) * rows].astype(f32) for k in range(width)],
                    axis=1,
                )
                for j in range(e * per, (e + 1) * per)
            ],
            axis=0,
        )
        outs.append(dot(inner.astype(bf16), down_ref[e]).astype(bf16))
    out_ref[...] = dot(back_ref[...], jnp.concatenate(outs, axis=0)).astype(bf16)
    normed = rounded(centred_ref[...] * inv_ref[...] * gain_ref[...])
    lane = iota((rows, lanes), 1)
    tiles = []
    for t in range(hidden // lanes):
        tile = jnp.zeros((rows, lanes), f32)
        for k in range(lanes // share):
            piece = inner_ref[t * (lanes // share) + k, width * rows :].astype(f32)
            turned = [
                pltpu.roll(piece, (k - b) * share % lanes, 1) for b in range(rows // 8)
            ]
            tile = jnp.where(lane // share == k, jnp.concatenate(turned, axis=0), tile)
        tiles.append(tile)
    shared = jnp.concatenate(tiles, axis=1).astype(bf16)
    base_ref[...] = res_scale * normed + dot(shared, shared_ref[...])


def combine(got_ref, high_ref, low_ref, base_ref, resid_ref, stats_ref):
    got = got_ref[...]
    resid = base_ref[...] + dot(high_ref[...], got) + dot(low_ref[...], got)
    resid_ref[...] = resid
    column = jnp.sum(resid, axis=1, keepdims=True)
    squares = jnp.sum(resid * resid, axis=1, keepdims=True)
    at, lane = iota(resid.shape, 0), iota(resid.shape, 1)
    half = lanes // 2
    seen = jnp.where(lane == at, column, jnp.where(lane == at + half, squares, 0.0))
    row = jnp.sum(seen, axis=0, keepdims=True)
    for j in range(stats_ref.shape[0]):
        stats_ref[j] = row


def finish(got_ref, resid_ref, gain_ref, out_ref, width):
    total = jnp.sum(got_ref[...], axis=0)
    at, lane = iota(resid_ref.shape, 0), iota(resid_ref.shape, 1)

    def column(start):
        return jnp.sum(jnp.where(lane == at + start, total, 0.0), axis=1, keepdims=True)

    mean = column(0) / width
    spread = column(lanes // 2) / width - mean * mean
    out_ref[...] = (
        (resid_ref[...] - mean) * lax.rsqrt(spread + norm_eps) * gain_ref[...]
    ).astype(bf16)


def to_each(value, axis):
    return lax.all_to_all(value, axis, split_axis=0, concat_axis=0, tiled=True)


def per_device(
    tokens,
    state,
    w_query,
    w_key,
    w_value,
    w_outgate,
    decay_down,
    decay_up,
    decay_bias,
    head_gain,
    w_output,
    norm1_gain,
    route_ids,
    route_weight,
    exp_gate,
    exp_up,
    exp_down,
    sh_gate,
    sh_up,
    sh_down,
    norm2_gain,
):
    rows, width = tokens.shape
    tp_count, ep_count = lax.axis_size("tp"), lax.axis_size("ep")
    cols = width // tp_count
    hidden = exp_gate.shape[2]
    per_block = exp_gate.shape[0] * capacity
    slots = ep_count * per_block
    gain1, gain2 = norm1_gain.reshape(1, cols), norm2_gain.reshape(1, cols)

    held = (
        route_ids.T,
        route_weight.T,
        tokens,
        decay_down.T,
        decay_up,
        decay_bias.reshape(1, -1),
        w_query,
        w_key,
        w_value,
        w_outgate,
        head_gain.reshape(1, -1),
        state,
        w_output,
    )
    later = (exp_gate, exp_up, sh_gate, sh_up)
    outgoing, send, high, low, perm, back, own, *later = local_call(
        attend,
        (
            struct((tp_count, rows + 8, cols), bf16),
            struct((slots, lanes), bf16),
            struct((rows, slots), bf16),
            struct((rows, slots), bf16),
            struct((slots, slots), bf16),
            struct((slots, slots), bf16),
            struct((rows, cols), f32),
            *(struct(a.shape, a.dtype) for a in later),
        ),
        held + later,
        stay=tuple(range(len(held + later))),
        scratch=[pltpu.VMEM(a.shape, a.dtype) for a in held]
        + [pltpu.SemaphoreType.DMA((len(held + later) + 1,))],
    )
    arrived = to_each(outgoing, "tp")

    def named(body):
        def call(*refs):
            body(*refs, width)

        call.__name__ = body.__name__
        return call

    sent, centred = local_call(
        named(dispatch),
        (struct((slots, cols), bf16), struct((rows, cols), f32)),
        (arrived, own, gain1, send),
    )
    taken = to_each(sent.reshape(ep_count, per_block, cols), "ep").reshape(slots, cols)
    tiles = hidden // lanes
    block = struct((tp_count // 2, 2 * tiles * rows + 16, lanes), bf16)
    keep, give = local_call(
        expand,
        (block, block),
        (taken, perm, *later, gain1, centred),
    )
    other = lax.ppermute(give, "tp", [(i, i ^ 1) for i in range(tp_count)])
    partials = local_call(pair, block, (keep, other))
    same_core = [list(range(core, tp_count, 2)) for core in range(2)]
    parts = lax.all_to_all(partials, "tp", 0, 0, tiled=True, axis_index_groups=same_core)
    inner, inv = local_call(
        named(activate),
        (struct((tiles * rows + 8, lanes), bf16), struct((rows, cols), f32)),
        (parts,),
    )
    inners = lax.all_gather(inner, "tp", axis=0)
    result, base = local_call(
        contract,
        (struct((slots, cols), bf16), struct((rows, cols), f32)),
        (inners, back, exp_down, sh_down, centred, gain1, inv),
    )
    returned = to_each(result.reshape(ep_count, per_block, cols), "ep").reshape(slots, cols)
    resid, stats = local_call(
        combine,
        (struct((rows, cols), f32), struct((tp_count, 1, lanes), f32)),
        (returned, high, low, base),
    )
    all_stats = to_each(stats, "tp")

    return local_call(
        named(finish), jax.ShapeDtypeStruct((rows, cols), bf16), (all_stats, resid, gain2)
    )


def solution(mesh):
    in_specs = (
        P("ep", None),
        P("ep", "tp", None, None),
        P(None, "tp"),
        P(None, "tp"),
        P(None, "tp"),
        P(None, "tp"),
        P(),
        P(None, "tp"),
        P("tp"),
        P(),
        P("tp", None),
        P("tp"),
        P("ep", None),
        P("ep", None),
        P("ep", "tp", None),
        P("ep", "tp", None),
        P("ep", None, "tp"),
        P("tp", None),
        P("tp", None),
        P(None, "tp"),
        P("tp"),
    )
    out_specs = P("ep", "tp")
    return jax.shard_map(
        per_device, mesh=mesh, in_specs=in_specs, out_specs=out_specs, check_vma=False
    )
```
